256 devices in a mesh: sp: 16 (over y, x), tp: 16 (over z, core).
Axes of the slice: x: 4, y: 4, z: 8, core: 2. Of those that a mesh axis runs over, the one named last changes fastest.
Arguments:
- lru_input: bfloat16 [4096, 2048], P('sp', 'tp'), may hold values from -27 to 27
- gate_input: bfloat16 [4096, 2048], P('sp', 'tp'), may hold values from -6 to 6
- documents: int32 [4096], P('sp'), may hold values from 0 to 3, never falling along the last dimension, each value on 1 to 1536 neighbouring positions
- conv_taps: bfloat16 [4, 2048], P(None, 'tp'), may hold values from -3 to 3
- rate_weight: bfloat16 [16, 128, 128], P('tp'), may hold values from -0.5 to 0.5
- inlet_weight: bfloat16 [16, 128, 128], P('tp'), may hold values from -0.5 to 0.5
- decay_param: float32 [2048], P('tp')
- lru_gain: float32 [2048], P('tp'), may hold values from 0.1 to 1.9
- out_weight: bfloat16 [2048, 2048], P('tp'), may hold values from -0.125 to 0.125
- residual: bfloat16 [4096, 2048], P('sp'), may hold values from -6 to 6
- ffn_gain: float32 [2048], replicated, may hold values from 0.1 to 1.9
- routes: int32 [4096, 2], P('sp'), may hold values from 0 to 15, all different within a row; in each aligned block of 16 rows (0 to 15, 16 to 31, ...) at most 4 rows name the same one
- route_weights: float32 [4096, 2], P('sp'), may hold values from 0.1 to 0.9
- w_gate: bfloat16 [16, 2048, 6144], P('sp', None, 'tp'), may hold values from -0.125 to 0.125
- w_up: bfloat16 [16, 2048, 6144], P('sp', None, 'tp'), may hold values from -0.125 to 0.125
- w_down: bfloat16 [16, 6144, 2048], P('sp', 'tp'), may hold values from -0.078125 to 0.078125
Outputs:
- mixed_out: bfloat16 [4096, 2048], P(('sp', 'tp'))
The draws below stay inside these ranges and needn't reach their ends.
Inputs may be any that keep to these rules, and one draw needn't show every extreme that they name: `documents`: document numbers start at 0 and never fall along the sequence; a document spans at most 1536 positions. `routes`: each row names 2 different experts. In each aligned block of 16 rows no expert is named by more than 4 rows, a bound that some block reaches.
All inputs are finite; a program needn't handle non-finite values.
Results may differ from the reference program's by a relative error of at most 0.017.
Values may be sent and summed in bfloat16 or wider, within the bound.
A program may use at most 64 MiB of HBM per device.

```python
import math
import jax
import jax.numpy as jnp
import numpy as np
from jax import lax

D = 2048
D_RNN = 2048
LRU_BLOCKS = 16
LRU_BLOCK = 128
CONV_TAPS = 4
FF = 6144
TOP = 2
TOKENS = 4096
ROUTE_ROWS = 16
EXPERTS = 16
CAP = 4
DOCS = 4
DOC_MOST = 1536
N_TP = 16


def draw_lru_input(key, part):
    base_key, group_key, span_key = jax.random.split(jax.random.fold_in(key, 11), 3)
    group_levels = jax.random.uniform(group_key, (LRU_BLOCKS,), jnp.float32, -1.2, 1.2)
    span_levels = jax.random.uniform(span_key, (TOKENS // 64,), jnp.float32, -0.7, 0.7)
    channel_scale = jnp.repeat(jnp.exp(group_levels), LRU_BLOCK)
    position_scale = jnp.repeat(jnp.exp(span_levels), 64)
    base_values = jnp.clip(jax.random.normal(base_key, (TOKENS, D_RNN), jnp.float32), -4.0, 4.0)
    return (base_values * channel_scale[None, :] * position_scale[:, None]).astype(jnp.bfloat16)


def draw_decay_param(key, part):
    pick_key, slow_key, fast_key = jax.random.split(jax.random.fold_in(key, 23), 3)
    slow_share = 0.5
    slow_pick = jax.random.uniform(pick_key, (D_RNN,), jnp.float32) < slow_share
    slow_value = math.log(2.5 * TOKENS) + jax.random.uniform(slow_key, (D_RNN,), jnp.float32, 0.0, 1.5)
    fast_value = jnp.log(jax.random.uniform(fast_key, (D_RNN,), jnp.float32, 120.0, 400.0))
    return jnp.where(slow_pick, slow_value, fast_value).astype(jnp.float32)


def block_levels(rng, extent, pieces, smallest, largest):
    level = 1.0
    for axis_at, parts in pieces:
        steps = jax.random.uniform(jax.random.fold_in(jax.random.fold_in(rng, 6), axis_at), (parts,), jnp.float32, smallest / len(pieces), largest / len(pieces))
        level = level * jnp.repeat(jnp.exp(steps), extent[axis_at] // parts).reshape((-1,) + (1,) * (len(extent) - 1 - axis_at))
    return level


def profile(number_of, total, reach, slope):
    weights = [(1 << 20) // math.isqrt(standing ** slope) + 1 for standing in range(2, number_of + 1)]
    surplus, counts = total - reach - (number_of - 1), [1] * (number_of - 1)
    while surplus > 0:
        movable = [i for i in range(number_of - 1) if counts[i] < reach]
        pool, budget = sum([weights[i] for i in movable]), surplus
        for i in movable:
            more = min(reach - counts[i], max(1, budget * weights[i] // pool), surplus)
            counts[i] = counts[i] + more
            surplus = surplus - more
    return np.array([reach] + counts)


def ragged_sizes(key, count, total, bound, lean):
    if count == 2:
        one = jax.random.randint(key, (), max(1, total - bound), min(bound, total - 1) + 1)
        return jnp.stack([one, total - one])
    lengths = jnp.asarray(profile(count, total, bound, lean), jnp.int32)
    twos = (count - 1) // 2
    donor, receiver = lengths[1:1 + 2 * twos:2], lengths[2:2 + 2 * twos:2]
    slack = jnp.minimum(donor - 1, bound - receiver)
    moved = jax.random.randint(jax.random.fold_in(key, 1), (twos,), 0, 1 << 20) % (slack + 1)
    lengths = lengths.at[1:1 + 2 * twos:2].set(donor - moved).at[2:2 + 2 * twos:2].set(receiver + moved)
    return lengths[jax.random.permutation(jax.random.fold_in(key, 2), count)]


def deal_out(key, own, number, rows, number_of, top, limit, lean):
    sequence = jax.random.permutation(key, number_of)
    packed, common = load_shares(number_of, rows * top, limit, lean, True), load_shares(number_of, rows * top, limit, lean, False)
    places = jnp.arange(number_of)

    def named(tallies, rotation):
        used = int((tallies > 0).sum())
        fixed = max(1, used // 4)
        passed = fixed + (places - fixed + rotation * (used - fixed)) % max(1, number_of - fixed)
        return jnp.zeros((number_of,), jnp.int32).at[sequence[jnp.where(places < fixed, places, passed)]].set(jnp.asarray(tallies, jnp.int32))

    tallies = jnp.where(number % 4 == 0, named(packed, number // 4), named(common, number - number // 4 - 1))
    mixed = jax.random.permutation(jax.random.fold_in(own, 3), number_of)
    donor, sink = mixed[0:number_of // 2 * 2:2], mixed[1:number_of // 2 * 2:2]
    room = jnp.minimum(tallies[donor] - 1, limit - tallies[sink]) // 2
    room = jnp.where((donor == sequence[0]) | (sink == sequence[0]) | (tallies[sink] == 0), 0, jnp.maximum(room, 0))
    passed = jax.random.randint(jax.random.fold_in(own, 4), (number_of // 2,), 0, 1 << 20) % (room + 1)
    tallies = tallies.at[donor].add(-passed).at[sink].add(passed)
    members = jnp.searchsorted(jnp.cumsum(tallies), jnp.arange(rows * top), side="right").astype(jnp.int32)
    listing = members.reshape(top, rows).T
    listing = listing[jax.random.permutation(jax.random.fold_in(own, 1), rows)]
    rotation = jax.random.randint(jax.random.fold_in(own, 2), (rows, 1), 0, top)
    return jnp.take_along_axis(listing, (jnp.arange(top)[None, :] + rotation) % top, axis=1)


def load_shares(number_of, total, reach, slope, full):
    weights = [(1 << 20) // math.isqrt(grade ** slope) + 1 for grade in range(1, number_of + 1)]
    largest = reach if full else min(reach, max(-(-total // number_of), total * weights[0] // sum(weights)))
    least = 1 if total - largest >= number_of - 1 else 0
    given, rest = [largest] + [least] * (number_of - 1), total - largest - least * (number_of - 1)
    while rest > 0:
        movable = [i for i in range(1, number_of) if given[i] < largest] or [i for i in range(1, number_of) if given[i] < reach]
        whole, left = sum([weights[i] for i in movable]), rest
        for i in movable:
            more = min(reach - given[i], max(1, left * weights[i] // whole), rest)
            given[i] = given[i] + more
            rest = rest - more
    return np.array(given)


def normal_values(stream_key, dims, deviation, limit, cuts=(), kind=jnp.bfloat16):
    values = deviation * jax.random.normal(stream_key, dims, jnp.float32)
    if cuts:
        values = values * block_levels(stream_key, dims, cuts, -0.22, 0.18)
    return jnp.clip(values, -limit, limit).astype(kind)


def setup_inputs(seed: int = 0) -> dict:
    arg_keys = jax.random.split(jax.random.key(seed), 17)
    lru_input = draw_lru_input(jax.random.fold_in(arg_keys[16], 71), 0)
    gate_input = normal_values(arg_keys[1], (TOKENS, D_RNN), 1.0, 6.0, ((0, 16), (1, 16)))
    documents = jnp.searchsorted(jnp.cumsum(ragged_sizes(arg_keys[2], DOCS, TOKENS, DOC_MOST, 0)), jnp.arange(TOKENS), side="right").astype(jnp.int32)
    conv_taps = normal_values(arg_keys[3], (CONV_TAPS, D_RNN), CONV_TAPS ** -0.5, 3.0, ((1, 16),))
    rate_weight = normal_values(arg_keys[4], (LRU_BLOCKS, LRU_BLOCK, LRU_BLOCK), LRU_BLOCK ** -0.5, 0.5, ((0, 16),))
    inlet_weight = normal_values(arg_keys[5], (LRU_BLOCKS, LRU_BLOCK, LRU_BLOCK), LRU_BLOCK ** -0.5, 0.5, ((0, 16),))
    decay_param = draw_decay_param(jax.random.fold_in(arg_keys[16], 71), 0)
    lru_gain = jnp.clip(1.0 + 0.18 * jax.random.normal(arg_keys[7], (D_RNN,), jnp.float32), 0.1, 1.9)
    out_weight = normal_values(arg_keys[8], (D_RNN, D), D_RNN ** -0.5, 0.125, ((0, 16),))
    residual = normal_values(arg_keys[9], (TOKENS, D), 1.0, 6.0, ((0, 16),))
    ffn_gain = jnp.clip(1.0 + 0.18 * jax.random.normal(arg_keys[10], (D,), jnp.float32), 0.1, 1.9)
    routes_keys = jax.random.split(jax.random.fold_in(arg_keys[11], 1), TOKENS // ROUTE_ROWS)
    routes_turns = jax.random.permutation(jax.random.fold_in(arg_keys[11], 3), TOKENS // ROUTE_ROWS)
    routes = jax.vmap(lambda own, number: deal_out(jax.random.fold_in(arg_keys[11], 2), own, number, ROUTE_ROWS, EXPERTS, TOP, CAP, 2))(routes_keys, routes_turns).reshape((TOKENS, TOP))
    route_weights = jnp.clip(0.1 + 0.79999997 * jax.random.uniform(arg_keys[12], (TOKENS, TOP), jnp.float32) ** block_levels(arg_keys[12], (TOKENS, TOP), ((0, 16),), -0.2, 0.2), 0.1, 0.9)
    w_gate = normal_values(arg_keys[13], (EXPERTS, D, FF), D ** -0.5, 0.125, ((0, 16), (2, 16)))
    w_up = normal_values(arg_keys[14], (EXPERTS, D, FF), D ** -0.5, 0.125, ((0, 16), (2, 16)))
    w_down = normal_values(arg_keys[15], (EXPERTS, FF, D), FF ** -0.5, 0.078125, ((0, 16), (1, 16)))
    return {"lru_input": lru_input, "gate_input": gate_input, "documents": documents, "conv_taps": conv_taps, "rate_weight": rate_weight, "inlet_weight": inlet_weight, "decay_param": decay_param, "lru_gain": lru_gain, "out_weight": out_weight, "residual": residual, "ffn_gain": ffn_gain, "routes": routes, "route_weights": route_weights, "w_gate": w_gate, "w_up": w_up, "w_down": w_down}


EPSILON = 1e-06
RATE_SCALE = 8.0

def join_runs(earlier_run, later_run):
    return (earlier_run[0] * later_run[0], later_run[0] * earlier_run[1] + later_run[1])

def slot_targets(route_block, expert_count, capacity):
    flat_routes = route_block.reshape(-1)
    onehot = (flat_routes[:, None] == jnp.arange(expert_count, dtype=jnp.int32)[None, :]).astype(jnp.int32)
    earlier_hits = jnp.cumsum(onehot, axis=0) - onehot
    slot_index = lax.optimization_barrier(jnp.sum(earlier_hits * onehot, axis=1))
    return (flat_routes * capacity + slot_index).astype(jnp.int32).reshape(route_block.shape)

def rms_rows(row_block, gain_vector):
    floated = row_block.astype(jnp.float32)
    inverse_rms = lax.rsqrt(lax.optimization_barrier(jnp.mean(floated * floated, axis=1, keepdims=True)) + EPSILON)
    return (floated * inverse_rms * gain_vector.astype(jnp.float32)[None, :]).astype(jnp.bfloat16)

def summed_blocks(left_rows, right_rows, blocks):
    span_width = left_rows.shape[1] // blocks

    def add_block(running, block_index):
        start_col = (block_index * span_width).astype(jnp.int32)
        partial_sum = jnp.dot(lax.dynamic_slice_in_dim(left_rows, start_col, span_width, 1), lax.dynamic_slice_in_dim(right_rows, start_col, span_width, 0), preferred_element_type=jnp.float32)
        partial_sum = lax.optimization_barrier(partial_sum.astype(jnp.bfloat16)).astype(jnp.float32)
        return (running + partial_sum, None)
    running, _ = lax.scan(add_block, jnp.zeros((left_rows.shape[0], right_rows.shape[1]), jnp.float32), jnp.arange(blocks, dtype=jnp.int32))
    return running

def reference(lru_input, gate_input, documents, conv_taps, rate_weight, inlet_weight, decay_param, lru_gain, out_weight, residual, ffn_gain, routes, route_weights, w_gate, w_up, w_down):
    documents = documents.astype(jnp.int32)
    reach_back = CONV_TAPS - 1
    prior_docs = jnp.concatenate([jnp.full((reach_back,), -1, jnp.int32), documents])
    padded_input = jnp.concatenate([jnp.zeros((reach_back, D_RNN), jnp.bfloat16), lru_input], axis=0)
    conv_sum = jnp.zeros((TOKENS, D_RNN), jnp.float32)
    for tap_index in range(CONV_TAPS):
        same_doc = (prior_docs[tap_index:tap_index + TOKENS] == documents).astype(jnp.float32)[:, None]
        conv_sum = conv_sum + padded_input[tap_index:tap_index + TOKENS].astype(jnp.float32) * conv_taps[tap_index].astype(jnp.float32)[None, :] * same_doc
    convolved = conv_sum.astype(jnp.bfloat16)
    grouped = convolved.astype(jnp.float32).reshape(TOKENS, LRU_BLOCKS, LRU_BLOCK)
    rate_gate = jax.nn.sigmoid(jnp.einsum('tnc,ncd->tnd', grouped, rate_weight.astype(jnp.float32)).reshape(TOKENS, D_RNN))
    inlet_gate = jax.nn.sigmoid(jnp.einsum('tnc,ncd->tnd', grouped, inlet_weight.astype(jnp.float32)).reshape(TOKENS, D_RNN))
    log_decay = -RATE_SCALE * rate_gate * jax.nn.softplus(-decay_param.astype(jnp.float32))[None, :]
    starts = (prior_docs[reach_back - 1:reach_back - 1 + TOKENS] != documents)[:, None]
    decay_step = jnp.where(starts, 0.0, jnp.exp(log_decay))
    norm_factor = jnp.where(starts, 1.0, jnp.sqrt(-jnp.expm1(2.0 * log_decay)))
    drive_term = norm_factor * inlet_gate * convolved.astype(jnp.float32)
    _, hidden_state = lax.associative_scan(join_runs, (decay_step, drive_term), axis=0)
    inverse_rms = lax.rsqrt(lax.optimization_barrier(jnp.mean(hidden_state * hidden_state, axis=1, keepdims=True)) + EPSILON)
    mixer_rows = (hidden_state * inverse_rms * lru_gain.astype(jnp.float32)[None, :] * jax.nn.gelu(gate_input.astype(jnp.float32))).astype(jnp.bfloat16)
    projected = summed_blocks(mixer_rows, out_weight, N_TP)
    after_mixer = (residual.astype(jnp.float32) + projected).astype(jnp.bfloat16)
    normed = rms_rows(after_mixer, ffn_gain)
    block_count = TOKENS // ROUTE_ROWS
    route_blocks = routes.astype(jnp.int32).reshape(block_count, ROUTE_ROWS, TOP)

    def block_slots(route_block):
        return slot_targets(route_block, EXPERTS, CAP)
    targets = jax.vmap(block_slots)(route_blocks)
    slot_index = targets - route_blocks * CAP
    block_ids = jnp.arange(block_count, dtype=jnp.int32)[:, None, None]
    buffer_rows = ((route_blocks * block_count + block_ids) * CAP + slot_index).astype(jnp.int32).reshape(-1)
    token_ids = jnp.broadcast_to(jnp.arange(TOKENS, dtype=jnp.int32).reshape(block_count, ROUTE_ROWS, 1), route_blocks.shape).reshape(-1)
    slot_table = jnp.zeros((EXPERTS * block_count * CAP,), jnp.int32).at[buffer_rows].set(token_ids + 1)
    padded_normed = jnp.concatenate([jnp.zeros((1, D), jnp.bfloat16), normed], axis=0)
    expert_span = block_count * CAP

    def run_expert(expert_id):
        picked_ids = lax.dynamic_slice_in_dim(slot_table, (expert_id * expert_span).astype(jnp.int32), expert_span, 0)
        expert_in = padded_normed[picked_ids]
        gate_part = jnp.dot(expert_in, w_gate[expert_id], preferred_element_type=jnp.float32)
        up_part = jnp.dot(expert_in, w_up[expert_id], preferred_element_type=jnp.float32)
        hidden_units = (jax.nn.silu(gate_part) * up_part).astype(jnp.bfloat16)
        return summed_blocks(hidden_units, w_down[expert_id], N_TP).astype(jnp.bfloat16)
    expert_out = lax.map(run_expert, jnp.arange(EXPERTS, dtype=jnp.int32))
    gathered = expert_out.reshape(EXPERTS * expert_span, D)[buffer_rows].astype(jnp.float32).reshape(TOKENS, TOP, D)
    routed = lax.optimization_barrier(jnp.sum(gathered * route_weights.astype(jnp.float32)[:, :, None], axis=1))
    return (after_mixer.astype(jnp.float32) + routed).astype(jnp.bfloat16)
```

```python
import functools

import jax
import jax.numpy as jnp
from jax import lax
from jax.experimental import pallas as pl
from jax.experimental.pallas import tpu as pltpu
from jax.sharding import PartitionSpec as P

MESH = pl.DeviceIdType.MESH
F32 = jnp.float32
BF16 = jnp.bfloat16
EPSILON = 1e-06
RATE_SCALE = 8.0
PARTS = 4
LANES = 128
REACH = 3
ROUTE_ROWS = 16


def softplus_of_minus(v):
    t = jnp.exp(-jnp.abs(v))
    s = t / (2.0 + t)
    s2 = s * s
    total = jnp.full_like(s, 1.0 / 19.0)
    for odd in (17, 15, 13, 11, 9, 7, 5, 3, 1):
        total = total * s2 + 1.0 / odd
    return jnp.maximum(-v, 0.0) + 2.0 * s * total


def one_minus_exp_of_minus(y, exp_minus_y):
    total = jnp.ones_like(y)
    for n in (8, 7, 6, 5, 4, 3, 2):
        total = 1.0 - y * (1.0 / n) * total
    return jnp.where(y < 0.5, y * total, 1.0 - exp_minus_y)


def gelu(v):
    return 0.5 * v * (1.0 + jnp.tanh(0.7978845608028654 * (v + 0.044715 * v * v * v)))


def iota(shape, dim):
    return lax.broadcasted_iota(jnp.int32, shape, dim)


def column_of(row, first, count):
    shape = (count, row.shape[1])
    return jnp.sum(
        jnp.where(iota(shape, 1) == iota(shape, 0) + first, row, 0.0), axis=1, keepdims=True
    )


def row_of(column, width):
    shape = (column.shape[0], width)
    return jnp.sum(jnp.where(iota(shape, 1) == iota(shape, 0), column, 0.0), axis=0, keepdims=True)


def kernel(
    n_sp,
    n_tp,
    lru,
    gate,
    docs,
    taps,
    rate,
    inlet,
    decay,
    gain,
    fgain,
    routes,
    rweights,
    w_out_hbm,
    resid_hbm,
    wg_hbm,
    wu_hbm,
    wd_hbm,
    out,
    xs,
    ds,
    a_s,
    b_s,
    hs,
    rx,
    cs,
    hd,
    w_out,
    resid,
    wg,
    wu,
    wd,
    sqb,
    sq2,
    pp,
    psib,
    pst,
    prp,
    prm,
    og,
    xg,
    po,
    sib,
    st,
    rp,
    rm,
    ret,
    rt,
    fo,
    fin,
    load_sem,
    fr_send,
    fr_recv,
    sq_send,
    sq_recv,
    s2_send,
    s2_recv,
    psib_send,
    psib_recv,
    prp_send,
    prp_recv,
    prm_send,
    prm_recv,
    di_send,
    di_recv,
    agp_send,
    agp_recv,
    agm_send,
    agm_recv,
    ags_send,
    ags_recv,
    sib_send,
    sib_recv,
    rp_send,
    rp_recv,
    rm_send,
    rm_recv,
    ret_send,
    ret_recv,
    fin_send,
    fin_recv,
):
    positions = lru.shape[0]
    model = wg.shape[0]
    width = model // PARTS
    n_z = n_tp // 2
    hops = n_z // 2
    quads = n_tp // PARTS
    tokens = positions // quads
    slot_rows = rt.shape[1]
    cap = slot_rows // PARTS
    half_slots = n_sp * slot_rows // 2
    half_tokens = tokens // 2
    s_me = lax.axis_index("sp")
    t_me = lax.axis_index("tp")
    z_me = lax.div(t_me, 2)
    c_me = lax.rem(t_me, 2)
    q_me = lax.div(t_me, PARTS)
    p_me = lax.rem(t_me, PARTS)
    sibling = z_me * 2 + (1 - c_me)
    up = lax.rem(z_me + 1, n_z) * 2 + c_me
    down = lax.rem(z_me + n_z - 1, n_z) * 2 + c_me

    def sp_peer(d):
        return lax.rem(s_me + d, n_sp)

    def tp_peer(d):
        return lax.rem(t_me + d, n_tp)

    def remote(src, dst, send, recv, **where):
        return pltpu.make_async_remote_copy(
            src_ref=src,
            dst_ref=dst,
            send_sem=send,
            recv_sem=recv,
            device_id=where,
            device_id_type=MESH,
        )

    def cols(part):
        return pl.ds(pl.multiple_of(part * width, LANES), width)

    def rows(start, size):
        return pl.ds(pl.multiple_of(start, 8), size)

    barrier = pltpu.get_barrier_semaphore()
    for d in range(1, n_sp):
        pl.semaphore_signal(barrier, inc=1, device_id={"sp": sp_peer(d)}, device_id_type=MESH)
    for d in range(1, n_tp):
        pl.semaphore_signal(barrier, inc=1, device_id={"tp": tp_peer(d)}, device_id_type=MESH)

    loads = [
        pltpu.make_async_copy(w_out_hbm, w_out, load_sem.at[0]),
        pltpu.make_async_copy(
            resid_hbm.at[rows(q_me * tokens, tokens), cols(p_me)], resid, load_sem.at[1]
        ),
        pltpu.make_async_copy(wg_hbm, wg, load_sem.at[2]),
        pltpu.make_async_copy(wu_hbm, wu, load_sem.at[3]),
        pltpu.make_async_copy(wd_hbm, wd, load_sem.at[4]),
    ]
    for load in loads:
        load.start()

    softplus = softplus_of_minus(decay[...])
    tap = [taps[k : k + 1, :].astype(F32) for k in range(REACH + 1)]

    def gates(convolved, starts):
        rate_gate = jax.nn.sigmoid(jnp.dot(convolved, rate[...], preferred_element_type=F32))
        inlet_gate = jax.nn.sigmoid(jnp.dot(convolved, inlet[...], preferred_element_type=F32))
        log_decay = -RATE_SCALE * rate_gate * softplus
        step = jnp.exp(log_decay)
        norm = jnp.sqrt(one_minus_exp_of_minus(-2.0 * log_decay, step * step))
        norm = jnp.where(starts, 1.0, norm)
        return jnp.where(starts, 0.0, step), norm * inlet_gate * convolved.astype(F32)

    doc_col = jnp.broadcast_to(
        column_of(docs[...].astype(F32), 0, positions), (positions, LANES)
    )
    x = lru[...].astype(F32)
    xs[0:8, :] = jnp.zeros((8, LANES), F32)
    xs[pl.ds(8, positions), :] = x
    ds[0:8, :] = jnp.full((8, LANES), -1.0, F32)
    ds[pl.ds(8, positions), :] = doc_col
    conv = jnp.zeros((positions, LANES), F32)
    for k in range(REACH + 1):
        back = 8 - REACH + k
        same = ds[pl.ds(back, positions), :] == doc_col
        conv = conv + jnp.where(same, xs[pl.ds(back, positions), :] * tap[k], 0.0)
    step, drive = gates(conv.astype(BF16), ds[pl.ds(7, positions), :] != doc_col)
    head = iota((positions, LANES), 0) < REACH
    step = jnp.where(head, 1.0, step)
    drive = jnp.where(head, 0.0, drive)
    run = positions // 8
    pitch = run + 8
    for j in range(8):
        a_s[pl.ds(j * pitch, run), :] = step[j * run : (j + 1) * run, :]
        b_s[pl.ds(j * pitch, run), :] = drive[j * run : (j + 1) * run, :]
    total_a = a_s[pl.ds(0, 8, stride=pitch), :]
    total_b = b_s[pl.ds(0, 8, stride=pitch), :]
    for i in range(1, run):
        here = a_s[pl.ds(i, 8, stride=pitch), :]
        total_b = here * total_b + b_s[pl.ds(i, 8, stride=pitch), :]
        total_a = here * total_a
        a_s[pl.ds(i, 8, stride=pitch), :] = total_a
        b_s[pl.ds(i, 8, stride=pitch), :] = total_b
    ahead_a = [jnp.ones((1, LANES), F32)]
    ahead_b = [jnp.zeros((1, LANES), F32)]
    for j in range(8):
        ahead_b.append(total_a[j : j + 1, :] * ahead_b[j] + total_b[j : j + 1, :])
        ahead_a.append(total_a[j : j + 1, :] * ahead_a[j])

    rx[0:16, :] = jnp.where(iota((16, LANES), 0) < 8, 0.0, jnp.full((16, LANES), -1.0, F32))
    own = pl.multiple_of((s_me + 1) * 16, 16)
    last = 8 + positions - REACH
    rx[pl.ds(own, 1), :] = ahead_a[8]
    rx[pl.ds(own + 1, 1), :] = ahead_b[8]
    rx[pl.ds(own + 2, REACH), :] = xs[8 : 8 + REACH, :]
    rx[pl.ds(own + 5, REACH), :] = xs[last : last + REACH, :]
    rx[pl.ds(own + 8, REACH), :] = ds[8 : 8 + REACH, :]
    rx[pl.ds(own + 11, REACH), :] = ds[last : last + REACH, :]
    rx[pl.ds(own + 14, 2), :] = jnp.zeros((2, LANES), F32)

    pl.semaphore_wait(barrier, n_sp + n_tp - 2)

    def front_copy(d, source):
        block = rx.at[rows((source + 1) * 16, 16), :]
        return remote(block, block, fr_send.at[d], fr_recv.at[source], sp=sp_peer(d))

    for d in range(1, n_sp):
        front_copy(d, s_me).start()
    gelu_gain = gelu(gate[...].astype(F32)) * gain[...]
    for d in range(1, n_sp):
        front_copy(d, sp_peer(d)).wait_recv()

    seq = [rx[pl.ds(5 + k, n_sp, stride=16), :] for k in range(REACH)]
    seq += [rx[pl.ds(18 + k, n_sp, stride=16), :] for k in range(REACH)]
    dseq = [rx[pl.ds(11 + k, n_sp, stride=16), :] for k in range(REACH)]
    dseq += [rx[pl.ds(24 + k, n_sp, stride=16), :] for k in range(REACH)]
    head_a, head_b = [], []
    for k in range(REACH):
        conv = jnp.zeros((n_sp, LANES), F32)
        for m in range(REACH + 1):
            conv = conv + jnp.where(dseq[k + m] == dseq[k + REACH], seq[k + m] * tap[m], 0.0)
        one_a, one_b = gates(conv.astype(BF16), dseq[k + REACH] != dseq[k + REACH - 1])
        head_a.append(one_a)
        head_b.append(one_b)
        hd[pl.ds(2 * k * n_sp, n_sp), :] = one_a
        hd[pl.ds((2 * k + 1) * n_sp, n_sp), :] = one_b
    body_a = rx[pl.ds(16, n_sp, stride=16), :]
    body_b = rx[pl.ds(17, n_sp, stride=16), :]
    all_b = (head_b[0] * head_a[1] + head_b[1]) * head_a[2] + head_b[2]
    cs[0:n_sp, :] = head_a[0] * head_a[1] * head_a[2] * body_a
    cs[n_sp : 2 * n_sp, :] = all_b * body_a + body_b
    state = jnp.zeros((1, LANES), F32)
    for s in range(n_sp - 1):
        state = jnp.where(s < s_me, cs[s : s + 1, :] * state + cs[n_sp + s : n_sp + s + 1, :], state)
    first = []
    for k in range(REACH):
        state = hd[pl.ds(2 * k * n_sp + s_me, 1), :] * state + hd[
            pl.ds((2 * k + 1) * n_sp + s_me, 1), :
        ]
        first.append(state)
    for j in range(8):
        carry = ahead_b[j] + ahead_a[j] * state
        piece = b_s[pl.ds(j * pitch, run), :] + a_s[pl.ds(j * pitch, run), :] * carry
        if j == 0:
            at = iota((run, LANES), 0)
            piece = jnp.where(at == 0, first[0], jnp.where(at == 1, first[1], piece))
        hs[pl.ds(j * run, run), :] = piece
    hidden = hs[...]

    sqb[pl.ds(t_me, 1), :, :] = row_of(
        jnp.sum(hidden * hidden, axis=1, keepdims=True), positions
    ).reshape(1, 1, positions)

    def square_copy(d, source):
        return remote(
            sqb.at[source], sqb.at[source], sq_send.at[d], sq_recv.at[source], tp=tp_peer(d)
        )

    mixer = (hidden * gelu_gain).astype(BF16)
    loads[0].wait()
    for part in range(PARTS):
        block = jnp.dot(
            mixer, w_out[:, part * width : (part + 1) * width], preferred_element_type=F32
        ).astype(BF16)
        for q in range(quads):
            pp[q, :, part * width : (part + 1) * width] = block[q * tokens : (q + 1) * tokens, :]
    for d in range(1, n_tp):
        square_copy(d, t_me).start()

    def to_sibling(src, dst, send, recv, q):
        copies = []
        for j in range(2):
            chip = 2 * q + j
            copies.append(
                remote(
                    src.at[q, :, cols(2 * j + 1 - c_me)],
                    dst.at[chip],
                    send.at[chip],
                    recv.at[chip],
                    tp=sibling,
                )
            )
        return copies

    def reduce_scatter(src, sib_buf, stage, buf_p, buf_m, sems, half):
        sib_s, sib_r, p_s, p_r, m_s, m_r = sems
        arrived = []

        def chip_at(offset):
            return lax.rem(z_me + offset + 2 * n_z, n_z)

        def wait_sibling(chip):
            remote(
                sib_buf.at[chip], sib_buf.at[chip], sib_s.at[chip], sib_r.at[chip], tp=sibling
            ).wait_recv()

        def term(chip, h):
            at = pl.ds(h * half, half)
            mine = src[lax.div(chip, 2), at, cols(lax.rem(chip, 2) * 2 + c_me)]
            return mine.astype(F32) + sib_buf[chip, at, :].astype(F32)

        def length(direction, h):
            return hops if (direction > 0) == (h == 0) else hops - 1

        def hop(direction, h, j, source):
            buf = buf_p if direction > 0 else buf_m
            sends, recvs = (p_s, p_r) if direction > 0 else (m_s, m_r)
            target = up if direction > 0 else down
            return remote(
                source, buf.at[h, j - 1], sends.at[h, j - 1], recvs.at[h, j - 1], tp=target
            )

        def arrival(direction, h, j):
            buf = buf_p if direction > 0 else buf_m
            return buf.at[h, j - 1]

        lanes = [(1, 0), (-1, 1), (1, 1), (-1, 0)]
        wait_sibling(chip_at(hops))
        for n, (direction, h) in enumerate(lanes):
            if n == 2:
                wait_sibling(chip_at(hops - 1))
                if hops > 1:
                    wait_sibling(chip_at(1 - hops))
            if length(direction, h) == 0:
                continue
            stage[n] = term(chip_at(direction * length(direction, h)), h).astype(BF16)
            hop(direction, h, 1, stage.at[n]).start()
        for d in range(hops - 2, -1, -1):
            wait_sibling(chip_at(d))
            if d > 0:
                wait_sibling(chip_at(-d))

        def step_of(j, _):
            for direction, h in lanes:
                n = length(direction, h)

                def one(direction=direction, h=h, n=n):
                    slot = arrival(direction, h, j - 1)
                    hop(direction, h, j - 1, slot).wait_recv()
                    value = term(chip_at(direction * (n + 1 - j)), h) + slot[...].astype(F32)
                    slot[...] = value.astype(BF16)
                    hop(direction, h, j, slot).start()

                if n == hops:
                    one()
                else:
                    pl.when(j < hops)(one)
            return 0

        lax.fori_loop(2, hops + 1, step_of, 0)
        for h in range(2):
            total = term(z_me, h)
            for direction in (1, -1):
                n = length(direction, h)
                if n:
                    slot = arrival(direction, h, n)
                    hop(direction, h, n, slot).wait_recv()
                    total = total + slot[...].astype(F32)
            arrived.append(total)
        for n, (direction, h) in enumerate(lanes):
            for j in range(1, length(direction, h) + 1):
                hop(direction, h, j, arrival(direction, h, j)).wait_send()
        return arrived

    copies = []
    for q in range(quads):
        copies += to_sibling(pp, psib, psib_send, psib_recv, q)
    for copy in copies:
        copy.start()
    parts = reduce_scatter(
        pp,
        psib,
        pst,
        prp,
        prm,
        (psib_send, psib_recv, prp_send, prp_recv, prm_send, prm_recv),
        half_tokens,
    )
    for copy in copies:
        copy.wait_send()
    for d in range(1, n_tp):
        square_copy(d, tp_peer(d)).wait_recv()
    squares = sqb[0]
    for t in range(1, n_tp):
        squares = squares + sqb[t]
    inverse = lax.rsqrt(squares / (n_tp * LANES) + EPSILON)
    inverse = column_of(inverse, q_me * tokens, tokens)
    loads[1].wait()
    for h in range(2):
        at = slice(h * half_tokens, (h + 1) * half_tokens)
        resid[at, :] = (
            resid[at, :].astype(F32) + parts[h] * inverse[at, :]
        ).astype(BF16)
    after = resid[...].astype(F32)
    sq2[pl.ds(p_me, 1), :, :] = row_of(
        jnp.sum(after * after, axis=1, keepdims=True), LANES
    ).reshape(1, 1, LANES)

    def quad_peer(d):
        return lax.rem(p_me + d, PARTS)

    def norm_copy(d, source):
        return remote(
            sq2.at[source],
            sq2.at[source],
            s2_send.at[d],
            s2_recv.at[source],
            tp=q_me * PARTS + quad_peer(d),
        )

    for d in range(1, PARTS):
        norm_copy(d, p_me).start()

    slots = n_sp * slot_rows
    shape = (tokens, slots)
    lane, token = iota(shape, 1), iota(shape, 0)
    expert = lax.div(lane, slot_rows)
    block = lax.div(lax.rem(lane, slot_rows), cap)
    place = lax.rem(lane, cap).astype(F32)
    here = block == lax.div(token, ROUTE_ROWS)
    expert = expert.astype(F32)
    route_rows = routes[...].astype(F32)
    named = [
        here & (column_of(route_rows[k : k + 1, :], q_me * tokens, tokens) == expert)
        for k in range(2)
    ]
    chosen = jnp.where(named[0] | named[1], 1.0, 0.0)
    earlier = jnp.where(iota((tokens, tokens), 1) < iota((tokens, tokens), 0), 1.0, 0.0)
    rank = jnp.dot(earlier.astype(BF16), chosen.astype(BF16), preferred_element_type=F32)
    pick = jnp.where(rank == place, chosen, 0.0)
    weight = jnp.zeros(shape, F32)
    for k in range(2):
        own_weight = column_of(rweights[k : k + 1, :], q_me * tokens, tokens)
        weight = weight + jnp.where(named[k], own_weight * pick, 0.0)
    weight_high = weight.astype(BF16)
    weight_low = (weight - weight_high.astype(F32)).astype(BF16)
    scale = fgain[:, cols(p_me)]
    for d in range(1, PARTS):
        norm_copy(d, quad_peer(d)).wait_recv()
    squares = sq2[0] + sq2[1] + sq2[2] + sq2[3]
    inverse = column_of(lax.rsqrt(squares / model + EPSILON), 0, tokens)
    normed = (after * inverse * scale).astype(BF16)
    outgoing = lax.dot_general(
        pick.astype(BF16), normed, (((0,), (0,)), ((), ())), preferred_element_type=F32
    ).astype(BF16)
    og[...] = outgoing.reshape(n_sp, slot_rows, width)
    xg[q_me, rows(s_me * slot_rows, slot_rows), cols(p_me)] = og[s_me]

    def dispatch_copy(d, source, peer):
        return remote(
            og.at[peer],
            xg.at[q_me, rows(source * slot_rows, slot_rows), cols(p_me)],
            di_send.at[d],
            di_recv.at[source],
            sp=peer,
        )

    for d in range(1, n_sp):
        dispatch_copy(d, s_me, sp_peer(d)).start()

    def sub_block(chip, h, core):
        return xg.at[
            lax.div(chip, 2),
            pl.ds(h * half_slots, half_slots),
            cols(lax.rem(chip, 2) * 2 + core),
        ]

    def ring_copy(direction, h, k, chip):
        sends, recvs = (agp_send, agp_recv) if direction > 0 else (agm_send, agm_recv)
        view = sub_block(chip, h, c_me)
        return remote(
            view, view, sends.at[h, k], recvs.at[h, k], tp=up if direction > 0 else down
        )

    def across_copy(h, chip, core):
        view = sub_block(chip, h, core)
        return remote(view, view, ags_send.at[h, chip], ags_recv.at[h, chip], tp=sibling)

    def reach(direction, h):
        return hops if (direction > 0) == (h == 0) else hops - 1

    for h in range(2):
        for source in range(h * n_sp // 2, (h + 1) * n_sp // 2):
            @pl.when(source != s_me)
            def _(source=source):
                remote(
                    og.at[source],
                    xg.at[q_me, rows(source * slot_rows, slot_rows), cols(p_me)],
                    di_send.at[0],
                    di_recv.at[source],
                    sp=sp_peer(1),
                ).wait_recv()
        for direction in (1, -1):
            if reach(direction, h):
                ring_copy(direction, h, 0, z_me).start()
        across_copy(h, z_me, c_me).start()
    for load in loads[2:]:
        load.wait()
    turn = 2 * lax.rem(z_me, 2) - 1

    def gather_step(k, _):
        for direction, h in ((1, 0), (-1, 1), (1, 1), (-1, 0)):
            n = reach(direction, h)

            def arrive(direction=direction, h=h, n=n):
                chip = lax.rem(z_me - direction * k + 2 * n_z, n_z)
                ring_copy(direction, h, k - 1, chip).wait_recv()

                @pl.when(k < n)
                def _():
                    ring_copy(direction, h, k, chip).start()

                across_copy(h, chip, c_me).start()

            if n == hops:
                arrive()
            else:
                pl.when(k < hops)(arrive)
        far = lax.div(k, 2)
        offset = jnp.where(lax.rem(k, 2) == 0, turn * far, -turn * far)
        q = lax.rem(q_me + offset + 2 * quads, quads)
        for j in range(2):
            for h in range(2):
                across_copy(h, 2 * q + j, 1 - c_me).wait_recv()
        rows_in = xg[q]
        gate_part = jnp.dot(rows_in, wg[...], preferred_element_type=F32)
        up_part = jnp.dot(rows_in, wu[...], preferred_element_type=F32)
        units = (jax.nn.silu(gate_part) * up_part).astype(BF16)
        for part in range(PARTS):
            at = slice(part * width, (part + 1) * width)
            po[q, :, at] = jnp.dot(units, wd[:, at], preferred_element_type=F32).astype(BF16)
        for copy in to_sibling(po, sib, sib_send, sib_recv, q):
            copy.start()
        return 0

    lax.fori_loop(1, hops + 1, gather_step, 0)

    parts = reduce_scatter(
        po,
        sib,
        st,
        rp,
        rm,
        (sib_send, sib_recv, rp_send, rp_recv, rm_send, rm_recv),
        half_slots,
    )
    half_sp = n_sp // 2
    for h in range(2):
        ret[h * half_sp : (h + 1) * half_sp] = (
            parts[h].astype(BF16).reshape(half_sp, slot_rows, width)
        )
    rt[pl.ds(s_me, 1)] = ret[pl.ds(s_me, 1)]

    def return_copy(d, source, peer):
        return remote(
            ret.at[peer], rt.at[source], ret_send.at[d], ret_recv.at[source], sp=peer
        )

    for d in range(1, n_sp):
        return_copy(d, s_me, sp_peer(d)).start()
    for d in range(1, n_sp):
        return_copy(d, sp_peer(d), sp_peer(d)).wait_recv()
    back = rt[...].reshape(slots, width)
    routed = jnp.dot(weight_high, back, preferred_element_type=F32) + jnp.dot(
        weight_low, back, preferred_element_type=F32
    )
    fo[...] = (resid[...].astype(F32) + routed).astype(BF16).reshape(PARTS, ROUTE_ROWS, width)
    fin[pl.ds(p_me, 1)] = fo[pl.ds(p_me, 1)]

    def final_copy(d, source, peer):
        return remote(
            fo.at[peer],
            fin.at[source],
            fin_send.at[d],
            fin_recv.at[source],
            tp=q_me * PARTS + peer,
        )

    for d in range(1, PARTS):
        final_copy(d, p_me, quad_peer(d)).start()
    for d in range(1, PARTS):
        final_copy(d, quad_peer(d), quad_peer(d)).wait_recv()
    for part in range(PARTS):
        out[:, part * width : (part + 1) * width] = fin[part]

    for d in range(1, n_sp):
        front_copy(d, s_me).wait_send()
        dispatch_copy(d, s_me, sp_peer(d)).wait_send()
        return_copy(d, s_me, sp_peer(d)).wait_send()
    for d in range(1, n_tp):
        square_copy(d, t_me).wait_send()
    for d in range(1, PARTS):
        norm_copy(d, p_me).wait_send()
        final_copy(d, p_me, quad_peer(d)).wait_send()
    for h in range(2):
        for direction in (1, -1):
            for k in range(reach(direction, h)):
                ring_copy(direction, h, k, z_me).wait_send()
        for chip in range(n_z):
            across_copy(h, chip, c_me).wait_send()
    for q in range(quads):
        for copy in to_sibling(po, sib, sib_send, sib_recv, q):
            copy.wait_send()


def local(
    n_sp,
    n_tp,
    lru_input,
    gate_input,
    documents,
    conv_taps,
    rate_weight,
    inlet_weight,
    decay_param,
    lru_gain,
    out_weight,
    residual,
    ffn_gain,
    routes,
    route_weights,
    w_gate,
    w_up,
    w_down,
):
    positions, channels = lru_input.shape
    model = residual.shape[1]
    units = w_gate.shape[2]
    width = model // PARTS
    n_z = n_tp // 2
    hops = n_z // 2
    quads = n_tp // PARTS
    tokens = positions // quads
    cap = 2 * routes.shape[1] * ROUTE_ROWS // n_sp
    slot_rows = PARTS * cap
    block_rows = n_sp * slot_rows
    pitch = positions + 64
    vmem = pl.BlockSpec(memory_space=pltpu.VMEM)
    hbm = pl.BlockSpec(memory_space=pl.ANY)
    dma = pltpu.SemaphoreType.DMA
    scratch = [
        pltpu.VMEM((positions + 8, LANES), F32),
        pltpu.VMEM((positions + 8, LANES), F32),
        pltpu.VMEM((pitch, LANES), F32),
        pltpu.VMEM((pitch, LANES), F32),
        pltpu.VMEM((positions, LANES), F32),
        pltpu.VMEM(((n_sp + 1) * 16, LANES), F32),
        pltpu.VMEM((2 * n_sp, LANES), F32),
        pltpu.VMEM((6 * n_sp, LANES), F32),
        pltpu.VMEM((channels, model), BF16),
        pltpu.VMEM((tokens, width), BF16),
        pltpu.VMEM((model, units), BF16),
        pltpu.VMEM((model, units), BF16),
        pltpu.VMEM((units, model), BF16),
        pltpu.VMEM((n_tp, 1, positions), F32),
        pltpu.VMEM((PARTS, 1, LANES), F32),
        pltpu.VMEM((quads, tokens, model), BF16),
        pltpu.VMEM((n_z, tokens, width), BF16),
        pltpu.VMEM((4, tokens // 2, width), BF16),
        pltpu.VMEM((2, hops, tokens // 2, width), BF16),
        pltpu.VMEM((2, hops, tokens // 2, width), BF16),
        pltpu.VMEM((n_sp, slot_rows, width), BF16),
        pltpu.VMEM((quads, block_rows, model), BF16),
        pltpu.VMEM((quads, block_rows, model), BF16),
        pltpu.VMEM((n_z, block_rows, width), BF16),
        pltpu.VMEM((4, block_rows // 2, width), BF16),
        pltpu.VMEM((2, hops, block_rows // 2, width), BF16),
        pltpu.VMEM((2, hops, block_rows // 2, width), BF16),
        pltpu.VMEM((n_sp, slot_rows, width), BF16),
        pltpu.VMEM((n_sp, slot_rows, width), BF16),
        pltpu.VMEM((PARTS, ROUTE_ROWS, width), BF16),
        pltpu.VMEM((PARTS, ROUTE_ROWS, width), BF16),
        dma((5,)),
        dma((n_sp,)),
        dma((n_sp,)),
        dma((n_tp,)),
        dma((n_tp,)),
        dma((PARTS,)),
        dma((PARTS,)),
        dma((n_z,)),
        dma((n_z,)),
        dma((2, hops)),
        dma((2, hops)),
        dma((2, hops)),
        dma((2, hops)),
        dma((n_sp,)),
        dma((n_sp,)),
        dma((2, hops)),
        dma((2, hops)),
        dma((2, hops)),
        dma((2, hops)),
        dma((2, n_z)),
        dma((2, n_z)),
        dma((n_z,)),
        dma((n_z,)),
        dma((2, hops)),
        dma((2, hops)),
        dma((2, hops)),
        dma((2, hops)),
        dma((n_sp,)),
        dma((n_sp,)),
        dma((PARTS,)),
        dma((PARTS,)),
    ]
    return pl.pallas_call(
        functools.partial(kernel, n_sp, n_tp),
        out_shape=jax.ShapeDtypeStruct((positions // n_tp, model), BF16),
        in_specs=[vmem] * 11 + [hbm] * 5,
        out_specs=vmem,
        scratch_shapes=scratch,
        name="layer",
        compiler_params=pltpu.CompilerParams(
            collective_id=0, has_side_effects=True, vmem_limit_bytes=56 * 1024 * 1024
        ),
    )(
        lru_input,
        gate_input,
        documents.reshape(1, positions),
        conv_taps,
        rate_weight[0],
        inlet_weight[0],
        decay_param.reshape(1, channels),
        lru_gain.reshape(1, channels),
        ffn_gain.reshape(1, model),
        routes.T,
        route_weights.T,
        out_weight,
        residual,
        w_gate[0],
        w_up[0],
        w_down[0],
    )


def solution(mesh):
    return jax.shard_map(
        functools.partial(local, mesh.shape["sp"], mesh.shape["tp"]),
        mesh=mesh,
        in_specs=(
            P("sp", "tp"),
            P("sp", "tp"),
            P("sp"),
            P(None, "tp"),
            P("tp", None, None),
            P("tp", None, None),
            P("tp"),
            P("tp"),
            P("tp", None),
            P("sp", None),
            P(),
            P("sp", None),
            P("sp", None),
            P("sp", None, "tp"),
            P("sp", None, "tp"),
            P("sp", "tp", None),
        ),
        out_specs=P(("sp", "tp"), None),
        check_vma=False,
    )
```

```python
import functools

import jax
import jax.numpy as jnp
from jax import lax
from jax.experimental import pallas as pl
from jax.experimental.pallas import tpu as pltpu
from jax.sharding import PartitionSpec as P

MESH = pl.DeviceIdType.MESH
F32 = jnp.float32
BF16 = jnp.bfloat16
EPSILON = 1e-06
RATE_SCALE = 8.0
PARTS = 4
LANES = 128
REACH = 3
ROUTE_ROWS = 16


def softplus_of_minus(v):
    t = jnp.exp(-jnp.abs(v))
    s = t / (2.0 + t)
    s2 = s * s
    total = jnp.full_like(s, 1.0 / 19.0)
    for odd in (17, 15, 13, 11, 9, 7, 5, 3, 1):
        total = total * s2 + 1.0 / odd
    return jnp.maximum(-v, 0.0) + 2.0 * s * total


def one_minus_exp_of_minus(y, exp_minus_y):
    total = jnp.ones_like(y)
    for n in (8, 7, 6, 5, 4, 3, 2):
        total = 1.0 - y * (1.0 / n) * total
    return jnp.where(y < 0.5, y * total, 1.0 - exp_minus_y)


def gelu(v):
    return 0.5 * v * (1.0 + jnp.tanh(0.7978845608028654 * (v + 0.044715 * v * v * v)))


def iota(shape, dim):
    return lax.broadcasted_iota(jnp.int32, shape, dim)


def when(condition, body):
    if isinstance(condition, bool):
        if condition:
            body()
    else:
        pl.when(condition)(body)


def column_of(row, first, count):
    shape = (count, row.shape[1])
    return jnp.sum(
        jnp.where(iota(shape, 1) == iota(shape, 0) + first, row, 0.0), axis=1, keepdims=True
    )


def row_of(column, width):
    shape = (column.shape[0], width)
    return jnp.sum(jnp.where(iota(shape, 1) == iota(shape, 0), column, 0.0), axis=0, keepdims=True)


def kernel(
    n_sp,
    n_tp,
    lru,
    gate,
    docs,
    taps,
    rate,
    inlet,
    decay,
    gain,
    fgain,
    routes,
    rweights,
    w_out_hbm,
    resid_hbm,
    wg_hbm,
    wu_hbm,
    wd_hbm,
    out,
    xs,
    ds,
    a_s,
    b_s,
    hs,
    rx,
    cs,
    hd,
    w_out,
    resid,
    wg,
    wu,
    wd,
    sqb,
    sq2,
    pp,
    psib,
    pst,
    prp,
    prm,
    pk,
    wh,
    wl,
    og,
    xa,
    ox,
    xg,
    po,
    sib,
    xsib,
    xo,
    xi,
    co,
    hs_out,
    hp,
    hm,
    gs,
    st,
    rp,
    rm,
    ret,
    rt,
    fo,
    fin,
    load_sem,
    fr_send,
    fr_recv,
    sq_send,
    sq_recv,
    s2_send,
    s2_recv,
    psib_send,
    psib_recv,
    prp_send,
    prp_recv,
    prm_send,
    prm_recv,
    di_send,
    di_recv,
    agp_send,
    agp_recv,
    agm_send,
    agm_recv,
    ags_send,
    ags_recv,
    xap_send,
    xap_recv,
    xam_send,
    xam_recv,
    ox_send,
    ox_recv,
    xf_send,
    xf_recv,
    sib_send,
    sib_recv,
    xsib_send,
    xsib_recv,
    xo_send,
    xo_recv,
    hp_send,
    hp_recv,
    hm_send,
    hm_recv,
    rp_send,
    rp_recv,
    rm_send,
    rm_recv,
    ret_send,
    ret_recv,
    fin_send,
    fin_recv,
):
    positions = lru.shape[0]
    model = wg.shape[0]
    width = model // PARTS
    half_w = width // 2
    n_z = n_tp // 2
    hops = n_z // 2
    quads = n_tp // PARTS
    tokens = positions // quads
    slot_rows = rt.shape[1]
    cap = slot_rows // PARTS
    half_slots = n_sp * slot_rows // 2
    half_tokens = tokens // 2
    s_me = lax.axis_index("sp")
    t_me = lax.axis_index("tp")
    z_me = lax.div(t_me, 2)
    c_me = lax.rem(t_me, 2)
    q_me = lax.div(t_me, PARTS)
    p_me = lax.rem(t_me, PARTS)
    sibling = z_me * 2 + (1 - c_me)
    up = lax.rem(z_me + 1, n_z) * 2 + c_me
    down = lax.rem(z_me + n_z - 1, n_z) * 2 + c_me

    def sp_peer(d):
        return lax.rem(s_me + d, n_sp)

    def tp_peer(d):
        return lax.rem(t_me + d, n_tp)

    def remote(src, dst, send, recv, **where):
        return pltpu.make_async_remote_copy(
            src_ref=src,
            dst_ref=dst,
            send_sem=send,
            recv_sem=recv,
            device_id=where,
            device_id_type=MESH,
        )

    def cols(part):
        return pl.ds(pl.multiple_of(part * width, LANES), width)

    def z_cols(part):
        return pl.ds(pl.multiple_of(part * half_w, LANES), half_w)

    def x_cols(core):
        return pl.ds(pl.multiple_of(PARTS * half_w + core * width, LANES), width)

    def rows(start, size):
        return pl.ds(pl.multiple_of(start, 8), size)

    barrier = pltpu.get_barrier_semaphore()
    for d in range(1, n_sp):
        pl.semaphore_signal(barrier, inc=1, device_id={"sp": sp_peer(d)}, device_id_type=MESH)
    for d in range(1, n_tp):
        pl.semaphore_signal(barrier, inc=1, device_id={"tp": tp_peer(d)}, device_id_type=MESH)

    loads = [
        pltpu.make_async_copy(w_out_hbm, w_out, load_sem.at[0]),
        pltpu.make_async_copy(
            resid_hbm.at[rows(q_me * tokens, tokens), cols(p_me)], resid, load_sem.at[1]
        ),
    ]
    for part in range(PARTS):
        x_at = PARTS * half_w + (part % 2) * width + (part // 2) * half_w
        for source, target in ((part * width, part * half_w), (part * width + half_w, x_at)):
            source, target = pl.ds(source, half_w), pl.ds(target, half_w)
            for a, b in (
                (wg_hbm.at[source, :], wg.at[target, :]),
                (wu_hbm.at[source, :], wu.at[target, :]),
                (wd_hbm.at[:, source], wd.at[:, target]),
            ):
                loads.append(pltpu.make_async_copy(a, b, load_sem.at[len(loads)]))
    for load in loads:
        load.start()

    softplus = softplus_of_minus(decay[...])
    tap = [taps[k : k + 1, :].astype(F32) for k in range(REACH + 1)]

    def gates(convolved, starts):
        rate_gate = jax.nn.sigmoid(jnp.dot(convolved, rate[...], preferred_element_type=F32))
        inlet_gate = jax.nn.sigmoid(jnp.dot(convolved, inlet[...], preferred_element_type=F32))
        log_decay = -RATE_SCALE * rate_gate * softplus
        step = jnp.exp(log_decay)
        norm = jnp.sqrt(one_minus_exp_of_minus(-2.0 * log_decay, step * step))
        norm = jnp.where(starts, 1.0, norm)
        return jnp.where(starts, 0.0, step), norm * inlet_gate * convolved.astype(F32)

    doc_col = jnp.broadcast_to(
        column_of(docs[...].astype(F32), 0, positions), (positions, LANES)
    )
    x = lru[...].astype(F32)
    xs[0:8, :] = jnp.zeros((8, LANES), F32)
    xs[pl.ds(8, positions), :] = x
    ds[0:8, :] = jnp.full((8, LANES), -1.0, F32)
    ds[pl.ds(8, positions), :] = doc_col
    conv = jnp.zeros((positions, LANES), F32)
    for k in range(REACH + 1):
        back = 8 - REACH + k
        same = ds[pl.ds(back, positions), :] == doc_col
        conv = conv + jnp.where(same, xs[pl.ds(back, positions), :] * tap[k], 0.0)
    step, drive = gates(conv.astype(BF16), ds[pl.ds(7, positions), :] != doc_col)
    head = iota((positions, LANES), 0) < REACH
    step = jnp.where(head, 1.0, step)
    drive = jnp.where(head, 0.0, drive)
    run = positions // 8
    pitch = run + 8
    for j in range(8):
        a_s[pl.ds(j * pitch, run), :] = step[j * run : (j + 1) * run, :]
        b_s[pl.ds(j * pitch, run), :] = drive[j * run : (j + 1) * run, :]
    total_a = a_s[pl.ds(0, 8, stride=pitch), :]
    total_b = b_s[pl.ds(0, 8, stride=pitch), :]
    for i in range(1, run):
        here = a_s[pl.ds(i, 8, stride=pitch), :]
        total_b = here * total_b + b_s[pl.ds(i, 8, stride=pitch), :]
        total_a = here * total_a
        a_s[pl.ds(i, 8, stride=pitch), :] = total_a
        b_s[pl.ds(i, 8, stride=pitch), :] = total_b
    ahead_a = [jnp.ones((1, LANES), F32)]
    ahead_b = [jnp.zeros((1, LANES), F32)]
    for j in range(8):
        ahead_b.append(total_a[j : j + 1, :] * ahead_b[j] + total_b[j : j + 1, :])
        ahead_a.append(total_a[j : j + 1, :] * ahead_a[j])

    rx[0:16, :] = jnp.where(iota((16, LANES), 0) < 8, 0.0, jnp.full((16, LANES), -1.0, F32))
    own = pl.multiple_of((s_me + 1) * 16, 16)
    last = 8 + positions - REACH
    rx[pl.ds(own, 1), :] = ahead_a[8]
    rx[pl.ds(own + 1, 1), :] = ahead_b[8]
    rx[pl.ds(own + 2, REACH), :] = xs[8 : 8 + REACH, :]
    rx[pl.ds(own + 5, REACH), :] = xs[last : last + REACH, :]
    rx[pl.ds(own + 8, REACH), :] = ds[8 : 8 + REACH, :]
    rx[pl.ds(own + 11, REACH), :] = ds[last : last + REACH, :]
    rx[pl.ds(own + 14, 2), :] = jnp.zeros((2, LANES), F32)

    pl.semaphore_wait(barrier, n_sp + n_tp - 2)

    def front_copy(d, source):
        block = rx.at[rows((source + 1) * 16, 16), :]
        return remote(block, block, fr_send.at[d], fr_recv.at[source], sp=sp_peer(d))

    for d in range(1, n_sp):
        front_copy(d, s_me).start()
    gelu_gain = gelu(gate[...].astype(F32)) * gain[...]

    slots = n_sp * slot_rows
    shape = (tokens, slots)
    lane, token = iota(shape, 1), iota(shape, 0)
    expert = lax.div(lane, slot_rows).astype(F32)
    place = lax.rem(lane, cap).astype(F32)
    here = lax.div(lax.rem(lane, slot_rows), cap) == lax.div(token, ROUTE_ROWS)
    earlier = jnp.where(iota((tokens, tokens), 1) < iota((tokens, tokens), 0), 1.0, 0.0).astype(BF16)
    route_rows = routes[...].astype(F32)
    for q in range(quads):
        named = [
            here & (column_of(route_rows[k : k + 1, :], q * tokens, tokens) == expert)
            for k in range(2)
        ]
        chosen = jnp.where(named[0] | named[1], 1.0, 0.0)
        rank = jnp.dot(earlier, chosen.astype(BF16), preferred_element_type=F32)
        pick = jnp.where(rank == place, chosen, 0.0)
        weight = jnp.zeros(shape, F32)
        for k in range(2):
            own_weight = column_of(rweights[k : k + 1, :], q * tokens, tokens)
            weight = weight + jnp.where(named[k], own_weight * pick, 0.0)
        high = weight.astype(BF16)
        pk[q] = pick.astype(BF16)
        wh[q] = high
        wl[q] = (weight - high.astype(F32)).astype(BF16)
    for d in range(1, n_sp):
        front_copy(d, sp_peer(d)).wait_recv()

    seq = [rx[pl.ds(5 + k, n_sp, stride=16), :] for k in range(REACH)]
    seq += [rx[pl.ds(18 + k, n_sp, stride=16), :] for k in range(REACH)]
    dseq = [rx[pl.ds(11 + k, n_sp, stride=16), :] for k in range(REACH)]
    dseq += [rx[pl.ds(24 + k, n_sp, stride=16), :] for k in range(REACH)]
    head_a, head_b = [], []
    for k in range(REACH):
        conv = jnp.zeros((n_sp, LANES), F32)
        for m in range(REACH + 1):
            conv = conv + jnp.where(dseq[k + m] == dseq[k + REACH], seq[k + m] * tap[m], 0.0)
        one_a, one_b = gates(conv.astype(BF16), dseq[k + REACH] != dseq[k + REACH - 1])
        head_a.append(one_a)
        head_b.append(one_b)
        hd[pl.ds(2 * k * n_sp, n_sp), :] = one_a
        hd[pl.ds((2 * k + 1) * n_sp, n_sp), :] = one_b
    body_a = rx[pl.ds(16, n_sp, stride=16), :]
    body_b = rx[pl.ds(17, n_sp, stride=16), :]
    all_b = (head_b[0] * head_a[1] + head_b[1]) * head_a[2] + head_b[2]
    cs[0:n_sp, :] = head_a[0] * head_a[1] * head_a[2] * body_a
    cs[n_sp : 2 * n_sp, :] = all_b * body_a + body_b
    state = jnp.zeros((1, LANES), F32)
    for s in range(n_sp - 1):
        state = jnp.where(s < s_me, cs[s : s + 1, :] * state + cs[n_sp + s : n_sp + s + 1, :], state)
    first = []
    for k in range(REACH):
        state = hd[pl.ds(2 * k * n_sp + s_me, 1), :] * state + hd[
            pl.ds((2 * k + 1) * n_sp + s_me, 1), :
        ]
        first.append(state)
    for j in range(8):
        carry = ahead_b[j] + ahead_a[j] * state
        piece = b_s[pl.ds(j * pitch, run), :] + a_s[pl.ds(j * pitch, run), :] * carry
        if j == 0:
            at = iota((run, LANES), 0)
            piece = jnp.where(at == 0, first[0], jnp.where(at == 1, first[1], piece))
        hs[pl.ds(j * run, run), :] = piece
    hidden = hs[...]

    sqb[pl.ds(t_me, 1), :, :] = row_of(
        jnp.sum(hidden * hidden, axis=1, keepdims=True), positions
    ).reshape(1, 1, positions)

    def square_copy(d, source):
        return remote(
            sqb.at[source], sqb.at[source], sq_send.at[d], sq_recv.at[source], tp=tp_peer(d)
        )

    mixer = (hidden * gelu_gain).astype(BF16)
    loads[0].wait()
    for part in range(PARTS):
        block = jnp.dot(
            mixer, w_out[:, part * width : (part + 1) * width], preferred_element_type=F32
        ).astype(BF16)
        for q in range(quads):
            pp[q, :, part * width : (part + 1) * width] = block[q * tokens : (q + 1) * tokens, :]
    for d in range(1, n_tp):
        square_copy(d, t_me).start()

    def chip_at(offset):
        return lax.rem(z_me + offset + 2 * n_z, n_z)

    def to_sibling(src, dst, send, recv, q, at):
        copies = []
        for j in range(2):
            chip = 2 * q + j
            copies.append(
                remote(
                    src.at[q, :, at(2 * j + 1 - c_me)],
                    dst.at[chip],
                    send.at[chip],
                    recv.at[chip],
                    tp=sibling,
                )
            )
        return copies

    def reduce_scatter(src, sib_buf, stage, buf_p, buf_m, sems, half, column):
        sib_s, sib_r, p_s, p_r, m_s, m_r = sems

        def wait_sibling(chip):
            remote(
                sib_buf.at[chip], sib_buf.at[chip], sib_s.at[chip], sib_r.at[chip], tp=sibling
            ).wait_recv()

        def term(chip, h):
            at = pl.ds(h * half, half)
            mine = src[lax.div(chip, 2), at, column(lax.rem(chip, 2) * 2 + c_me)]
            return mine.astype(F32) + sib_buf[chip, at, :].astype(F32)

        def length(direction, h):
            return hops if (direction > 0) == (h == 0) else hops - 1

        def hop(direction, h, j, source):
            buf = buf_p if direction > 0 else buf_m
            sends, recvs = (p_s, p_r) if direction > 0 else (m_s, m_r)
            target = up if direction > 0 else down
            return remote(
                source, buf.at[h, j - 1], sends.at[h, j - 1], recvs.at[h, j - 1], tp=target
            )

        def arrival(direction, h, j):
            buf = buf_p if direction > 0 else buf_m
            return buf.at[h, j - 1]

        lanes = [(1, 0), (-1, 1), (1, 1), (-1, 0)]

        def begin():
            wait_sibling(chip_at(hops))
            for n, (direction, h) in enumerate(lanes):
                if n == 2:
                    wait_sibling(chip_at(hops - 1))
                    if hops > 1:
                        wait_sibling(chip_at(1 - hops))
                if length(direction, h) == 0:
                    continue
                stage[n] = term(chip_at(direction * length(direction, h)), h).astype(BF16)
                hop(direction, h, 1, stage.at[n]).start()
            for d in range(hops - 2, -1, -1):
                wait_sibling(chip_at(d))
                if d > 0:
                    wait_sibling(chip_at(-d))

        def step_of(j):
            for direction, h in lanes:
                n = length(direction, h)

                def one(direction=direction, h=h, n=n):
                    slot = arrival(direction, h, j - 1)
                    hop(direction, h, j - 1, slot).wait_recv()
                    value = term(chip_at(direction * (n + 1 - j)), h) + slot[...].astype(F32)
                    slot[...] = value.astype(BF16)
                    hop(direction, h, j, slot).start()

                when(j <= n if isinstance(j, int) else n == hops or j <= n, one)

        def result(h):
            total = term(z_me, h)
            for direction in (1, -1):
                n = length(direction, h)
                if n:
                    slot = arrival(direction, h, n)
                    hop(direction, h, n, slot).wait_recv()
                    total = total + slot[...].astype(F32)
            return total

        def drain():
            for n, (direction, h) in enumerate(lanes):
                for j in range(1, length(direction, h) + 1):
                    hop(direction, h, j, arrival(direction, h, j)).wait_send()

        return begin, step_of, result, drain

    copies = []
    for q in range(quads):
        copies += to_sibling(pp, psib, psib_send, psib_recv, q, cols)
    for copy in copies:
        copy.start()
    begin, step_of, result, drain_projection = reduce_scatter(
        pp,
        psib,
        pst,
        prp,
        prm,
        (psib_send, psib_recv, prp_send, prp_recv, prm_send, prm_recv),
        half_tokens,
        cols,
    )
    begin()

    def projection_step(j, _):
        step_of(j)
        return 0

    lax.fori_loop(2, hops + 1, projection_step, 0)
    parts = [result(h) for h in range(2)]
    for d in range(1, n_tp):
        square_copy(d, tp_peer(d)).wait_recv()
    squares = sqb[0]
    for t in range(1, n_tp):
        squares = squares + sqb[t]
    inverse = lax.rsqrt(squares / (n_tp * LANES) + EPSILON)
    inverse = column_of(inverse, q_me * tokens, tokens)
    loads[1].wait()
    for h in range(2):
        at = slice(h * half_tokens, (h + 1) * half_tokens)
        resid[at, :] = (
            resid[at, :].astype(F32) + parts[h] * inverse[at, :]
        ).astype(BF16)
    after = resid[...].astype(F32)
    sq2[pl.ds(p_me, 1), :, :] = row_of(
        jnp.sum(after * after, axis=1, keepdims=True), LANES
    ).reshape(1, 1, LANES)

    def quad_peer(d):
        return lax.rem(p_me + d, PARTS)

    def norm_copy(d, source):
        return remote(
            sq2.at[source],
            sq2.at[source],
            s2_send.at[d],
            s2_recv.at[source],
            tp=q_me * PARTS + quad_peer(d),
        )

    for d in range(1, PARTS):
        norm_copy(d, p_me).start()

    scale = fgain[:, cols(p_me)]
    for d in range(1, PARTS):
        norm_copy(d, quad_peer(d)).wait_recv()
    squares = sq2[0] + sq2[1] + sq2[2] + sq2[3]
    inverse = column_of(lax.rsqrt(squares / model + EPSILON), 0, tokens)
    normed = (after * inverse * scale).astype(BF16)
    turn = 2 * lax.rem(z_me, 2) - 1

    def quad_at(k):
        far = lax.div(k, 2)
        offset = jnp.where(lax.rem(k, 2) == 0, turn * far, -turn * far)
        return lax.rem(q_me + offset + 2 * quads, quads)

    xa[z_me] = normed[:, half_w:]

    def ahead_copy(direction, k, chip):
        sends, recvs = (xap_send, xap_recv) if direction > 0 else (xam_send, xam_recv)
        return remote(
            xa.at[chip],
            xa.at[chip],
            sends.at[k],
            recvs.at[k],
            tp=up if direction > 0 else down,
        )

    def ahead_step(k):
        for direction, n in ((1, hops), (-1, hops - 1)):

            def arrive(direction=direction, n=n):
                chip = chip_at(-direction * k)
                ahead_copy(direction, k - 1, chip).wait_recv()
                when(k < n, lambda: ahead_copy(direction, k, chip).start())

            when(k <= n, arrive)

    ahead_copy(1, 0, z_me).start()
    if hops > 1:
        ahead_copy(-1, 0, z_me).start()

    over_slots = (((0,), (0,)), ((), ()))
    outgoing = lax.dot_general(
        pk[q_me], normed[:, :half_w], over_slots, preferred_element_type=F32
    ).astype(BF16)
    og[...] = outgoing.reshape(n_sp, slot_rows, half_w)
    xg[q_me, rows(s_me * slot_rows, slot_rows), z_cols(p_me)] = og[s_me]

    def dispatch_copy(d, source, peer):
        return remote(
            og.at[peer],
            xg.at[q_me, rows(source * slot_rows, slot_rows), z_cols(p_me)],
            di_send.at[d],
            di_recv.at[source],
            sp=peer,
        )

    for d in range(1, n_sp):
        dispatch_copy(d, s_me, sp_peer(d)).start()

    def late_copy(q, d, source, peer):
        return remote(
            ox.at[q, peer],
            xg.at[q, rows(source * slot_rows, slot_rows), x_cols(c_me)],
            ox_send.at[q, d],
            ox_recv.at[q, source],
            sp=peer,
        )

    def send_quad(q):
        both = jnp.concatenate([xa[2 * q], xa[2 * q + 1]], axis=1)
        picked = lax.dot_general(pk[q], both, over_slots, preferred_element_type=F32)
        ox[q] = picked.astype(BF16).reshape(n_sp, slot_rows, width)
        xg[q, rows(s_me * slot_rows, slot_rows), x_cols(c_me)] = ox[q, s_me]

        def one(d, _):
            late_copy(q, d, s_me, sp_peer(d)).start()
            return 0

        lax.fori_loop(1, n_sp, one, 0)

    def sub_block(chip, h, core):
        return xg.at[
            lax.div(chip, 2),
            pl.ds(h * half_slots, half_slots),
            z_cols(lax.rem(chip, 2) * 2 + core),
        ]

    def ring_copy(direction, h, k, chip):
        sends, recvs = (agp_send, agp_recv) if direction > 0 else (agm_send, agm_recv)
        view = sub_block(chip, h, c_me)
        return remote(
            view, view, sends.at[h, k], recvs.at[h, k], tp=up if direction > 0 else down
        )

    def across_copy(h, chip, core):
        view = sub_block(chip, h, core)
        return remote(view, view, ags_send.at[h, chip], ags_recv.at[h, chip], tp=sibling)

    def across_late(q, core):
        view = xg.at[q, :, x_cols(core)]
        return remote(view, view, xf_send.at[q], xf_recv.at[q], tp=sibling)

    def reach(direction, h):
        return hops if (direction > 0) == (h == 0) else hops - 1

    ahead_step(1)
    send_quad(quad_at(1))
    ahead_step(2)
    send_quad(quad_at(2))
    for h in range(2):
        for source in range(h * n_sp // 2, (h + 1) * n_sp // 2):

            @pl.when(source != s_me)
            def _(source=source):
                dispatch_copy(0, source, source).wait_recv()

        for direction in (1, -1):
            if reach(direction, h):
                ring_copy(direction, h, 0, z_me).start()
        across_copy(h, z_me, c_me).start()
    for load in loads[2:]:
        load.wait()

    def forward(k, h):
        for direction in (1, -1) if h == 0 else (-1, 1):
            n = reach(direction, h)

            def arrive(direction=direction, n=n):
                chip = chip_at(-direction * k)
                ring_copy(direction, h, k - 1, chip).wait_recv()

                @pl.when(k < n)
                def _():
                    ring_copy(direction, h, k, chip).start()

                across_copy(h, chip, c_me).start()

            pl.when(k <= n)(arrive)

    def forward_late(q):
        def one(d, _):
            late_copy(q, 0, sp_peer(d), sp_peer(d)).wait_recv()
            return 0

        lax.fori_loop(1, n_sp, one, 0)
        across_late(q, c_me).start()

    def late_to_sibling(q):
        return remote(
            po.at[q, :, x_cols(1 - c_me)],
            xsib.at[q],
            xsib_send.at[q],
            xsib_recv.at[q],
            tp=sibling,
        )

    def out_to_sibling(q):
        return [late_to_sibling(q)] + to_sibling(po, sib, sib_send, sib_recv, q, z_cols)

    def experts_gate(q):
        for j in range(2):
            for h in range(2):
                across_copy(h, 2 * q + j, 1 - c_me).wait_recv()
        across_late(q, 1 - c_me).wait_recv()
        gs[...] = jax.nn.silu(jnp.dot(xg[q], wg[...], preferred_element_type=F32))

    def experts(q):
        up_part = jnp.dot(xg[q], wu[...], preferred_element_type=F32)
        units = (gs[...] * up_part).astype(BF16)
        for part in range(PARTS):
            at = slice(part * width, (part + 1) * width)
            po[q, :, at] = jnp.dot(units, wd[:, at], preferred_element_type=F32).astype(BF16)
        for copy in out_to_sibling(q):
            copy.start()

    def early_copy(q, d, source, peer):
        return remote(
            xo.at[q, peer], xi.at[q, source], xo_send.at[q, d], xo_recv.at[q, source], sp=peer
        )

    def return_early(q):
        late_to_sibling(q).wait_recv()
        total = po[q, :, x_cols(c_me)].astype(F32) + xsib[q].astype(F32)
        xo[q] = total.astype(BF16).reshape(n_sp, slot_rows, width)
        xi[q, pl.ds(s_me, 1)] = xo[q, pl.ds(s_me, 1)]

        def one(d, _):
            early_copy(q, d, s_me, sp_peer(d)).start()
            return 0

        lax.fori_loop(1, n_sp, one, 0)

    def weigh(q, back):
        return jnp.dot(wh[q], back, preferred_element_type=F32) + jnp.dot(
            wl[q], back, preferred_element_type=F32
        )

    def weigh_early(q):
        def one(d, _):
            early_copy(q, 0, sp_peer(d), sp_peer(d)).wait_recv()
            return 0

        lax.fori_loop(1, n_sp, one, 0)
        total = weigh(q, xi[q].reshape(slots, width))
        for j in range(2):
            co[2 * q + j] = total[:, j * half_w : (j + 1) * half_w]

    def home_copy(direction, j, source):
        sends, recvs, slot = (hp_send, hp_recv, hp) if direction > 0 else (hm_send, hm_recv, hm)
        return remote(
            source,
            slot.at[j - 1],
            sends.at[j - 1],
            recvs.at[j - 1],
            tp=up if direction > 0 else down,
        )

    ways = [(1, hops, hp), (-1, hops - 1, hm)]

    def home_step(j):
        for direction, n, slots_in in ways:
            if j > n:
                continue
            value = co[chip_at(direction * (n + 1 - j))]
            if j == 1:
                source = hs_out.at[0 if direction > 0 else 1]
            else:
                source = slots_in.at[j - 2]
                home_copy(direction, j - 1, source).wait_recv()
                value = value + source[...].astype(F32)
            source[...] = value.astype(BF16)
            home_copy(direction, j, source).start()

    def home_result():
        total = co[z_me]
        for direction, n, slots_in in ways:
            if n:
                home_copy(direction, n, slots_in.at[n - 1]).wait_recv()
                total = total + slots_in[n - 1].astype(F32)
        return total

    def gather_step(k, _):
        @pl.when(k <= hops - 2)
        def _():
            ahead_step(k + 2)
            send_quad(quad_at(k + 2))

        @pl.when(k <= hops)
        def _():
            forward(k, 0)

        @pl.when(k >= 2)
        def _():
            experts_gate(quad_at(k - 1))

        @pl.when(k <= hops)
        def _():
            forward(k, 1)
            forward_late(quad_at(k))

        @pl.when(k >= 2)
        def _():
            experts(quad_at(k - 1))

        @pl.when(k >= 3)
        def _():
            return_early(quad_at(k - 2))

        return 0

    lax.fori_loop(1, hops + 2, gather_step, 0)

    begin, step_of, result, drain_experts = reduce_scatter(
        po,
        sib,
        st,
        rp,
        rm,
        (sib_send, sib_recv, rp_send, rp_recv, rm_send, rm_recv),
        half_slots,
        z_cols,
    )
    begin()
    return_early(quad_at(hops))

    homeward = 0
    for j in range(2, hops + 1):
        step_of(j)
        if homeward:
            homeward += 1
            home_step(homeward)
        for k in range(2 * j - 3, min(2 * j - 1, hops + 1)):
            weigh_early(quad_at(k))
            if k == hops:
                homeward = 1
                home_step(1)
    half_sp = n_sp // 2

    def return_copy(d, source, peer):
        return remote(
            ret.at[peer], rt.at[source], ret_send.at[d], ret_recv.at[source], sp=peer
        )

    for h in range(2):
        ret[h * half_sp : (h + 1) * half_sp] = (
            result(h).astype(BF16).reshape(half_sp, slot_rows, half_w)
        )
    rt[pl.ds(s_me, 1)] = ret[pl.ds(s_me, 1)]
    for d in range(1, n_sp):
        return_copy(d, s_me, sp_peer(d)).start()
    for j in range(homeward + 1, hops + 1):
        home_step(j)
    for d in range(1, n_sp):
        return_copy(d, sp_peer(d), sp_peer(d)).wait_recv()
    routed = weigh(q_me, rt[...].reshape(slots, half_w))
    fo[:, :, :half_w] = (
        (resid[:, :half_w].astype(F32) + routed)
        .astype(BF16)
        .reshape(PARTS, ROUTE_ROWS, half_w)
    )
    routed = home_result()
    fo[:, :, half_w:] = (
        (resid[:, half_w:].astype(F32) + routed)
        .astype(BF16)
        .reshape(PARTS, ROUTE_ROWS, half_w)
    )
    fin[pl.ds(p_me, 1)] = fo[pl.ds(p_me, 1)]

    def final_copy(d, source, peer):
        return remote(
            fo.at[peer],
            fin.at[source],
            fin_send.at[d],
            fin_recv.at[source],
            tp=q_me * PARTS + peer,
        )

    for d in range(1, PARTS):
        final_copy(d, p_me, quad_peer(d)).start()
    for d in range(1, PARTS):
        final_copy(d, quad_peer(d), quad_peer(d)).wait_recv()
    for part in range(PARTS):
        out[:, part * width : (part + 1) * width] = fin[part]

    for d in range(1, n_sp):
        front_copy(d, s_me).wait_send()
        dispatch_copy(d, s_me, sp_peer(d)).wait_send()
        return_copy(d, s_me, sp_peer(d)).wait_send()
    for d in range(1, n_tp):
        square_copy(d, t_me).wait_send()
    for d in range(1, PARTS):
        norm_copy(d, p_me).wait_send()
        final_copy(d, p_me, quad_peer(d)).wait_send()
    for h in range(2):
        for direction in (1, -1):
            for k in range(reach(direction, h)):
                ring_copy(direction, h, k, z_me).wait_send()
        for chip in range(n_z):
            across_copy(h, chip, c_me).wait_send()
    for copy in copies:
        copy.wait_send()
    drain_projection()
    drain_experts()
    for direction, n, slots_in in ways:
        for k in range(n):
            ahead_copy(direction, k, z_me).wait_send()
            home_copy(direction, k + 1, slots_in.at[k]).wait_send()
    for q in range(quads):
        across_late(q, c_me).wait_send()
        for copy in out_to_sibling(q):
            copy.wait_send()

        def one(d, _, q=q):
            late_copy(q, d, s_me, sp_peer(d)).wait_send()
            early_copy(q, d, s_me, sp_peer(d)).wait_send()
            return 0

        lax.fori_loop(1, n_sp, one, 0)

def local(
    n_sp,
    n_tp,
    lru_input,
    gate_input,
    documents,
    conv_taps,
    rate_weight,
    inlet_weight,
    decay_param,
    lru_gain,
    out_weight,
    residual,
    ffn_gain,
    routes,
    route_weights,
    w_gate,
    w_up,
    w_down,
):
    positions, channels = lru_input.shape
    model = residual.shape[1]
    units = w_gate.shape[2]
    width = model // PARTS
    half_w = width // 2
    n_z = n_tp // 2
    hops = n_z // 2
    quads = n_tp // PARTS
    tokens = positions // quads
    cap = 2 * routes.shape[1] * ROUTE_ROWS // n_sp
    slot_rows = PARTS * cap
    block_rows = n_sp * slot_rows
    pitch = positions + 64
    vmem = pl.BlockSpec(memory_space=pltpu.VMEM)
    hbm = pl.BlockSpec(memory_space=pl.ANY)
    dma = pltpu.SemaphoreType.DMA
    scratch = [
        pltpu.VMEM((positions + 8, LANES), F32),
        pltpu.VMEM((positions + 8, LANES), F32),
        pltpu.VMEM((pitch, LANES), F32),
        pltpu.VMEM((pitch, LANES), F32),
        pltpu.VMEM((positions, LANES), F32),
        pltpu.VMEM(((n_sp + 1) * 16, LANES), F32),
        pltpu.VMEM((2 * n_sp, LANES), F32),
        pltpu.VMEM((6 * n_sp, LANES), F32),
        pltpu.VMEM((channels, model), BF16),
        pltpu.VMEM((tokens, width), BF16),
        pltpu.VMEM((model, units), BF16),
        pltpu.VMEM((model, units), BF16),
        pltpu.VMEM((units, model), BF16),
        pltpu.VMEM((n_tp, 1, positions), F32),
        pltpu.VMEM((PARTS, 1, LANES), F32),
        pltpu.VMEM((quads, tokens, model), BF16),
        pltpu.VMEM((n_z, tokens, width), BF16),
        pltpu.VMEM((4, tokens // 2, width), BF16),
        pltpu.VMEM((2, hops, tokens // 2, width), BF16),
        pltpu.VMEM((2, hops, tokens // 2, width), BF16),
        pltpu.VMEM((quads, tokens, block_rows), BF16),
        pltpu.VMEM((quads, tokens, block_rows), BF16),
        pltpu.VMEM((quads, tokens, block_rows), BF16),
        pltpu.VMEM((n_sp, slot_rows, half_w), BF16),
        pltpu.VMEM((n_z, tokens, half_w), BF16),
        pltpu.VMEM((quads, n_sp, slot_rows, width), BF16),
        pltpu.VMEM((quads, block_rows, model), BF16),
        pltpu.VMEM((quads, block_rows, model), BF16),
        pltpu.VMEM((n_z, block_rows, half_w), BF16),
        pltpu.VMEM((quads, block_rows, width), BF16),
        pltpu.VMEM((quads, n_sp, slot_rows, width), BF16),
        pltpu.VMEM((quads, n_sp, slot_rows, width), BF16),
        pltpu.VMEM((n_z, tokens, half_w), F32),
        pltpu.VMEM((2, tokens, half_w), BF16),
        pltpu.VMEM((hops, tokens, half_w), BF16),
        pltpu.VMEM((hops, tokens, half_w), BF16),
        pltpu.VMEM((block_rows, units), F32),
        pltpu.VMEM((4, block_rows // 2, half_w), BF16),
        pltpu.VMEM((2, hops, block_rows // 2, half_w), BF16),
        pltpu.VMEM((2, hops, block_rows // 2, half_w), BF16),
        pltpu.VMEM((n_sp, slot_rows, half_w), BF16),
        pltpu.VMEM((n_sp, slot_rows, half_w), BF16),
        pltpu.VMEM((PARTS, ROUTE_ROWS, width), BF16),
        pltpu.VMEM((PARTS, ROUTE_ROWS, width), BF16),
        dma((2 + 6 * PARTS,)),
        dma((n_sp,)),
        dma((n_sp,)),
        dma((n_tp,)),
        dma((n_tp,)),
        dma((PARTS,)),
        dma((PARTS,)),
        dma((n_z,)),
        dma((n_z,)),
        dma((2, hops)),
        dma((2, hops)),
        dma((2, hops)),
        dma((2, hops)),
        dma((n_sp,)),
        dma((n_sp,)),
        dma((2, hops)),
        dma((2, hops)),
        dma((2, hops)),
        dma((2, hops)),
        dma((2, n_z)),
        dma((2, n_z)),
        dma((hops,)),
        dma((hops,)),
        dma((hops,)),
        dma((hops,)),
        dma((quads, n_sp)),
        dma((quads, n_sp)),
        dma((quads,)),
        dma((quads,)),
        dma((n_z,)),
        dma((n_z,)),
        dma((quads,)),
        dma((quads,)),
        dma((quads, n_sp)),
        dma((quads, n_sp)),
        dma((hops,)),
        dma((hops,)),
        dma((hops,)),
        dma((hops,)),
        dma((2, hops)),
        dma((2, hops)),
        dma((2, hops)),
        dma((2, hops)),
        dma((n_sp,)),
        dma((n_sp,)),
        dma((PARTS,)),
        dma((PARTS,)),
    ]
    return pl.pallas_call(
        functools.partial(kernel, n_sp, n_tp),
        out_shape=jax.ShapeDtypeStruct((positions // n_tp, model), BF16),
        in_specs=[vmem] * 11 + [hbm] * 5,
        out_specs=vmem,
        scratch_shapes=scratch,
        name="layer",
        compiler_params=pltpu.CompilerParams(
            collective_id=0, has_side_effects=True, vmem_limit_bytes=56 * 1024 * 1024
        ),
    )(
        lru_input,
        gate_input,
        documents.reshape(1, positions),
        conv_taps,
        rate_weight[0],
        inlet_weight[0],
        decay_param.reshape(1, channels),
        lru_gain.reshape(1, channels),
        ffn_gain.reshape(1, model),
        routes.T,
        route_weights.T,
        out_weight,
        residual,
        w_gate[0],
        w_up[0],
        w_down[0],
    )


def solution(mesh):
    return jax.shard_map(
        functools.partial(local, mesh.shape["sp"], mesh.shape["tp"]),
        mesh=mesh,
        in_specs=(
            P("sp", "tp"),
            P("sp", "tp"),
            P("sp"),
            P(None, "tp"),
            P("tp", None, None),
            P("tp", None, None),
            P("tp"),
            P("tp"),
            P("tp", None),
            P("sp", None),
            P(),
            P("sp", None),
            P("sp", None),
            P("sp", None, "tp"),
            P("sp", None, "tp"),
            P("sp", "tp", None),
        ),
        out_specs=P(("sp", "tp"), None),
        check_vma=False,
    )
```

```python
import functools

import jax
import jax.numpy as jnp
from jax import lax
from jax.experimental import pallas as pl
from jax.experimental.pallas import tpu as pltpu
from jax.sharding import PartitionSpec as P

MESH = pl.DeviceIdType.MESH
F32 = jnp.float32
BF16 = jnp.bfloat16
EPSILON = 1e-06
RATE_SCALE = 8.0
PARTS = 4
LANES = 128
REACH = 3
ROUTE_ROWS = 16
PIECES = 4


def softplus_of_minus(v):
    t = jnp.exp(-jnp.abs(v))
    s = t / (2.0 + t)
    s2 = s * s
    total = jnp.full_like(s, 1.0 / 19.0)
    for odd in (17, 15, 13, 11, 9, 7, 5, 3, 1):
        total = total * s2 + 1.0 / odd
    return jnp.maximum(-v, 0.0) + 2.0 * s * total


def one_minus_exp_of_minus(y, exp_minus_y):
    total = jnp.ones_like(y)
    for n in (8, 7, 6, 5, 4, 3, 2):
        total = 1.0 - y * (1.0 / n) * total
    return jnp.where(y < 0.5, y * total, 1.0 - exp_minus_y)


def gelu(v):
    return 0.5 * v * (1.0 + jnp.tanh(0.7978845608028654 * (v + 0.044715 * v * v * v)))


def iota(shape, dim):
    return lax.broadcasted_iota(jnp.int32, shape, dim)


def when(condition, body):
    if isinstance(condition, bool):
        if condition:
            body()
    else:
        pl.when(condition)(body)


def column_of(row, first, count):
    shape = (count, row.shape[1])
    return jnp.sum(
        jnp.where(iota(shape, 1) == iota(shape, 0) + first, row, 0.0), axis=1, keepdims=True
    )


def row_of(column, width):
    shape = (column.shape[0], width)
    return jnp.sum(jnp.where(iota(shape, 1) == iota(shape, 0), column, 0.0), axis=0, keepdims=True)


def kernel(
    n_sp,
    n_tp,
    lru_hbm,
    gate_hbm,
    docs_hbm,
    taps_hbm,
    rate_hbm,
    inlet_hbm,
    decay_hbm,
    gain_hbm,
    fgain_hbm,
    routes_hbm,
    rweights_hbm,
    w_out_hbm,
    resid_hbm,
    wg_hbm,
    wu_hbm,
    wd_hbm,
    out,
    lru,
    gate,
    docs,
    taps,
    rate,
    inlet,
    decay,
    gain,
    fgain,
    routes,
    rweights,
    in_sem,
    xs,
    ds,
    a_s,
    b_s,
    hs,
    rx,
    cs,
    hd,
    w_out,
    resid,
    wgu,
    wd,
    sqb,
    sq2,
    pp,
    psib,
    pst,
    prp,
    prm,
    pk,
    wh,
    wl,
    og,
    xa,
    ox,
    xg,
    po,
    sib,
    xsib,
    xo,
    xi,
    co,
    ci,
    gs,
    st,
    rp,
    rm,
    ret,
    rt,
    fo,
    fin,
    load_sem,
    fr_send,
    fr_recv,
    sq_send,
    sq_recv,
    s2_send,
    s2_recv,
    psib_send,
    psib_recv,
    prp_send,
    prp_recv,
    prm_send,
    prm_recv,
    di_send,
    di_recv,
    agp_send,
    agp_recv,
    agm_send,
    agm_recv,
    ags_send,
    ags_recv,
    xap_send,
    xap_recv,
    xam_send,
    xam_recv,
    ox_send,
    ox_recv,
    sib_send,
    sib_recv,
    xsib_send,
    xsib_recv,
    xo_send,
    xo_recv,
    co_send,
    co_recv,
    rp_send,
    rp_recv,
    rm_send,
    rm_recv,
    ret_send,
    ret_recv,
    fin_send,
    fin_recv,
):
    positions = lru.shape[0]
    model = wgu.shape[0]
    units_n = wd.shape[0]
    width = model // PARTS
    half_w = width // 2
    n_z = n_tp // 2
    hops = n_z // 2
    quads = n_tp // PARTS
    tokens = positions // quads
    slot_rows = rt.shape[1]
    cap = slot_rows // PARTS
    piece_slots = n_sp * slot_rows // PIECES
    half_tokens = tokens // 2
    s_me = lax.axis_index("sp")
    t_me = lax.axis_index("tp")
    z_me = lax.div(t_me, 2)
    c_me = lax.rem(t_me, 2)
    q_me = lax.div(t_me, PARTS)
    p_me = lax.rem(t_me, PARTS)
    sibling = z_me * 2 + (1 - c_me)
    up = lax.rem(z_me + 1, n_z) * 2 + c_me
    down = lax.rem(z_me + n_z - 1, n_z) * 2 + c_me

    def sp_peer(d):
        return lax.rem(s_me + d, n_sp)

    def tp_peer(d):
        return lax.rem(t_me + d, n_tp)

    def remote(src, dst, send, recv, **where):
        return pltpu.make_async_remote_copy(
            src_ref=src,
            dst_ref=dst,
            send_sem=send,
            recv_sem=recv,
            device_id=where,
            device_id_type=MESH,
        )

    def got(view, sem):
        remote(view, view, sem, sem, tp=sibling).wait_recv()

    def sent(view, sem):
        remote(view, view, sem, sem, tp=sibling).wait_send()

    def cols(part):
        return pl.ds(pl.multiple_of(part * width, LANES), width)

    def z_cols(part):
        return pl.ds(pl.multiple_of(part * half_w, LANES), half_w)

    def x_cols(core):
        return pl.ds(pl.multiple_of(PARTS * half_w + core * width, LANES), width)

    def rows(start, size):
        return pl.ds(pl.multiple_of(start, 8), size)

    inputs = [
        pltpu.make_async_copy(lru_hbm, lru, in_sem.at[0]),
        pltpu.make_async_copy(gate_hbm, gate, in_sem.at[1]),
        pltpu.make_async_copy(docs_hbm, docs, in_sem.at[2]),
        pltpu.make_async_copy(taps_hbm, taps, in_sem.at[3]),
        pltpu.make_async_copy(rate_hbm, rate, in_sem.at[4]),
        pltpu.make_async_copy(inlet_hbm, inlet, in_sem.at[5]),
        pltpu.make_async_copy(decay_hbm, decay, in_sem.at[6]),
        pltpu.make_async_copy(gain_hbm, gain, in_sem.at[7]),
        pltpu.make_async_copy(fgain_hbm, fgain, in_sem.at[8]),
        pltpu.make_async_copy(routes_hbm, routes, in_sem.at[9]),
        pltpu.make_async_copy(rweights_hbm, rweights, in_sem.at[10]),
    ]
    for copy in inputs:
        copy.start()
    barrier = pltpu.get_barrier_semaphore()
    for d in range(1, n_sp):
        pl.semaphore_signal(barrier, inc=1, device_id={"sp": sp_peer(d)}, device_id_type=MESH)
    for d in range(1, n_tp):
        pl.semaphore_signal(barrier, inc=1, device_id={"tp": tp_peer(d)}, device_id_type=MESH)

    loads = [
        pltpu.make_async_copy(w_out_hbm, w_out, load_sem.at[0]),
        pltpu.make_async_copy(
            resid_hbm.at[rows(q_me * tokens, tokens), cols(p_me)], resid, load_sem.at[1]
        ),
    ]
    for part in range(PARTS):
        x_at = PARTS * half_w + (part % 2) * width + (part // 2) * half_w
        for source, target in ((part * width, part * half_w), (part * width + half_w, x_at)):
            source, target = pl.ds(source, half_w), pl.ds(target, half_w)
            for a, b in (
                (wg_hbm.at[source, :], wgu.at[target, pl.ds(0, units_n)]),
                (wu_hbm.at[source, :], wgu.at[target, pl.ds(units_n, units_n)]),
            ):
                loads.append(pltpu.make_async_copy(a, b, load_sem.at[2]))
            loads.append(
                pltpu.make_async_copy(wd_hbm.at[:, source], wd.at[:, target], load_sem.at[3])
            )
    for copy in inputs:
        copy.wait()
    for load in loads:
        load.start()

    softplus = softplus_of_minus(decay[...])
    tap = [taps[k : k + 1, :].astype(F32) for k in range(REACH + 1)]

    def gates(convolved, starts):
        rate_gate = jax.nn.sigmoid(jnp.dot(convolved, rate[...], preferred_element_type=F32))
        inlet_gate = jax.nn.sigmoid(jnp.dot(convolved, inlet[...], preferred_element_type=F32))
        log_decay = -RATE_SCALE * rate_gate * softplus
        step = jnp.exp(log_decay)
        norm = jnp.sqrt(one_minus_exp_of_minus(-2.0 * log_decay, step * step))
        norm = jnp.where(starts, 1.0, norm)
        return jnp.where(starts, 0.0, step), norm * inlet_gate * convolved.astype(F32)

    doc_col = jnp.broadcast_to(
        column_of(docs[...].astype(F32), 0, positions), (positions, LANES)
    )
    x = lru[...].astype(F32)
    xs[0:8, :] = jnp.zeros((8, LANES), F32)
    xs[pl.ds(8, positions), :] = x
    ds[0:8, :] = jnp.full((8, LANES), -1.0, F32)
    ds[pl.ds(8, positions), :] = doc_col
    conv = jnp.zeros((positions, LANES), F32)
    for k in range(REACH + 1):
        back = 8 - REACH + k
        same = ds[pl.ds(back, positions), :] == doc_col
        conv = conv + jnp.where(same, xs[pl.ds(back, positions), :] * tap[k], 0.0)
    step, drive = gates(conv.astype(BF16), ds[pl.ds(7, positions), :] != doc_col)
    head = iota((positions, LANES), 0) < REACH
    step = jnp.where(head, 1.0, step)
    drive = jnp.where(head, 0.0, drive)
    run = positions // 8
    pitch = run + 8
    for j in range(8):
        a_s[pl.ds(j * pitch, run), :] = step[j * run : (j + 1) * run, :]
        b_s[pl.ds(j * pitch, run), :] = drive[j * run : (j + 1) * run, :]
    total_a = a_s[pl.ds(0, 8, stride=pitch), :]
    total_b = b_s[pl.ds(0, 8, stride=pitch), :]
    for i in range(1, run):
        here = a_s[pl.ds(i, 8, stride=pitch), :]
        total_b = here * total_b + b_s[pl.ds(i, 8, stride=pitch), :]
        total_a = here * total_a
        a_s[pl.ds(i, 8, stride=pitch), :] = total_a
        b_s[pl.ds(i, 8, stride=pitch), :] = total_b
    ahead_a = [jnp.ones((1, LANES), F32)]
    ahead_b = [jnp.zeros((1, LANES), F32)]
    for j in range(8):
        ahead_b.append(total_a[j : j + 1, :] * ahead_b[j] + total_b[j : j + 1, :])
        ahead_a.append(total_a[j : j + 1, :] * ahead_a[j])

    rx[0:16, :] = jnp.where(iota((16, LANES), 0) < 8, 0.0, jnp.full((16, LANES), -1.0, F32))
    own = pl.multiple_of((s_me + 1) * 16, 16)
    last = 8 + positions - REACH
    rx[pl.ds(own, 1), :] = ahead_a[8]
    rx[pl.ds(own + 1, 1), :] = ahead_b[8]
    rx[pl.ds(own + 2, REACH), :] = xs[8 : 8 + REACH, :]
    rx[pl.ds(own + 5, REACH), :] = xs[last : last + REACH, :]
    rx[pl.ds(own + 8, REACH), :] = ds[8 : 8 + REACH, :]
    rx[pl.ds(own + 11, REACH), :] = ds[last : last + REACH, :]
    rx[pl.ds(own + 14, 2), :] = jnp.zeros((2, LANES), F32)

    pl.semaphore_wait(barrier, n_sp + n_tp - 2)

    def front_copy(d, source):
        block = rx.at[rows((source + 1) * 16, 16), :]
        return remote(block, block, fr_send, fr_recv, sp=sp_peer(d))

    for d in range(1, n_sp):
        front_copy(d, s_me).start()
    gelu_gain = gelu(gate[...].astype(F32)) * gain[...]

    slots = n_sp * slot_rows
    shape = (tokens, slots)
    lane, token = iota(shape, 1), iota(shape, 0)
    expert = lax.div(lane, slot_rows).astype(F32)
    place = lax.rem(lane, cap).astype(F32)
    here = lax.div(lax.rem(lane, slot_rows), cap) == lax.div(token, ROUTE_ROWS)
    earlier = jnp.where(iota((tokens, tokens), 1) < iota((tokens, tokens), 0), 1.0, 0.0).astype(BF16)
    route_rows = routes[...].astype(F32)
    for q in range(quads):
        named = [
            here & (column_of(route_rows[k : k + 1, :], q * tokens, tokens) == expert)
            for k in range(2)
        ]
        chosen = jnp.where(named[0] | named[1], 1.0, 0.0)
        rank = jnp.dot(earlier, chosen.astype(BF16), preferred_element_type=F32)
        pick = jnp.where(rank == place, chosen, 0.0)
        weight = jnp.zeros(shape, F32)
        for k in range(2):
            own_weight = column_of(rweights[k : k + 1, :], q * tokens, tokens)
            weight = weight + jnp.where(named[k], own_weight * pick, 0.0)
        high = weight.astype(BF16)
        pk[q] = pick.astype(BF16)
        wh[q] = high
        wl[q] = (weight - high.astype(F32)).astype(BF16)
    got(rx.at[: (n_sp - 1) * 16, :], fr_recv)

    seq = [rx[pl.ds(5 + k, n_sp, stride=16), :] for k in range(REACH)]
    seq += [rx[pl.ds(18 + k, n_sp, stride=16), :] for k in range(REACH)]
    dseq = [rx[pl.ds(11 + k, n_sp, stride=16), :] for k in range(REACH)]
    dseq += [rx[pl.ds(24 + k, n_sp, stride=16), :] for k in range(REACH)]
    head_a, head_b = [], []
    for k in range(REACH):
        conv = jnp.zeros((n_sp, LANES), F32)
        for m in range(REACH + 1):
            conv = conv + jnp.where(dseq[k + m] == dseq[k + REACH], seq[k + m] * tap[m], 0.0)
        one_a, one_b = gates(conv.astype(BF16), dseq[k + REACH] != dseq[k + REACH - 1])
        head_a.append(one_a)
        head_b.append(one_b)
        hd[pl.ds(2 * k * n_sp, n_sp), :] = one_a
        hd[pl.ds((2 * k + 1) * n_sp, n_sp), :] = one_b
    body_a = rx[pl.ds(16, n_sp, stride=16), :]
    body_b = rx[pl.ds(17, n_sp, stride=16), :]
    all_b = (head_b[0] * head_a[1] + head_b[1]) * head_a[2] + head_b[2]
    cs[0:n_sp, :] = head_a[0] * head_a[1] * head_a[2] * body_a
    cs[n_sp : 2 * n_sp, :] = all_b * body_a + body_b
    state = jnp.zeros((1, LANES), F32)
    for s in range(n_sp - 1):
        state = jnp.where(s < s_me, cs[s : s + 1, :] * state + cs[n_sp + s : n_sp + s + 1, :], state)
    first = []
    for k in range(REACH):
        state = hd[pl.ds(2 * k * n_sp + s_me, 1), :] * state + hd[
            pl.ds((2 * k + 1) * n_sp + s_me, 1), :
        ]
        first.append(state)
    for j in range(8):
        carry = ahead_b[j] + ahead_a[j] * state
        piece = b_s[pl.ds(j * pitch, run), :] + a_s[pl.ds(j * pitch, run), :] * carry
        if j == 0:
            at = iota((run, LANES), 0)
            piece = jnp.where(at == 0, first[0], jnp.where(at == 1, first[1], piece))
        hs[pl.ds(j * run, run), :] = piece
    hidden = hs[...]

    sqb[pl.ds(t_me, 1), :, :] = row_of(
        jnp.sum(hidden * hidden, axis=1, keepdims=True), positions
    ).reshape(1, 1, positions)

    def square_copy(d, source):
        return remote(
            sqb.at[source], sqb.at[source], sq_send, sq_recv, tp=tp_peer(d)
        )

    mixer = (hidden * gelu_gain).astype(BF16)
    loads[0].wait()
    for part in range(PARTS):
        block = jnp.dot(
            mixer, w_out[:, part * width : (part + 1) * width], preferred_element_type=F32
        ).astype(BF16)
        for q in range(quads):
            pp[q, :, part * width : (part + 1) * width] = block[q * tokens : (q + 1) * tokens, :]
    for d in range(1, n_tp):
        square_copy(d, t_me).start()

    def chip_at(offset):
        return lax.rem(z_me + offset + 2 * n_z, n_z)

    def to_sibling(src, dst, send, recv, q, at):
        copies = []
        for j in range(2):
            chip = 2 * q + j
            copies.append(
                remote(
                    src.at[q, :, at(2 * j + 1 - c_me)],
                    dst.at[chip],
                    send,
                    recv.at[q],
                    tp=sibling,
                )
            )
        return copies

    def reduce_scatter(src, sib_buf, stage, buf_p, buf_m, sems, pieces, column):
        sib_r, p_s, p_r, m_s, m_r = sems
        half = src.shape[1] // pieces

        def term(chip, h):
            at = pl.ds(h * half, half)
            mine = src[lax.div(chip, 2), at, column(lax.rem(chip, 2) * 2 + c_me)]
            return mine.astype(F32) + sib_buf[chip, at, :].astype(F32)

        def length(direction, h):
            return hops if (direction > 0) == (h % 2 == 0) else hops - 1

        def hop(direction, h, j, source):
            buf = buf_p if direction > 0 else buf_m
            sends, recvs = (p_s, p_r) if direction > 0 else (m_s, m_r)
            target = up if direction > 0 else down
            return remote(
                source, buf.at[h * hops + j - 1], sends, recvs.at[h, j - 1], tp=target
            )

        def arrival(direction, h, j):
            buf = buf_p if direction > 0 else buf_m
            return buf.at[h * hops + j - 1]

        lanes = [(1 - 2 * (h % 2), h) for h in range(pieces)]
        lanes += [(2 * (h % 2) - 1, h) for h in range(pieces)]
        lanes = [lane for h in range(pieces) for lane in (lanes[h], lanes[h + pieces])]
        lanes.sort(key=lambda lane: (lane[1] // 2, -length(*lane)))

        def begin():
            for q in range(quads):
                got(sib_buf.at[2 * q : 2 * q + 2], sib_r.at[q])
            for n, (direction, h) in enumerate(lanes):
                if length(direction, h) == 0:
                    continue
                stage[n] = term(chip_at(direction * length(direction, h)), h).astype(BF16)
                hop(direction, h, 1, stage.at[n]).start()

        def step_of(j):
            for direction, h in lanes:
                n = length(direction, h)

                def one(direction=direction, h=h, n=n):
                    slot = arrival(direction, h, j - 1)
                    hop(direction, h, j - 1, slot).wait_recv()
                    value = term(chip_at(direction * (n + 1 - j)), h) + slot[...].astype(F32)
                    slot[...] = value.astype(BF16)
                    hop(direction, h, j, slot).start()

                when(j <= n if isinstance(j, int) else n == hops or j <= n, one)

        def result(h):
            total = term(z_me, h)
            for direction in (1, -1):
                n = length(direction, h)
                if n:
                    slot = arrival(direction, h, n)
                    hop(direction, h, n, slot).wait_recv()
                    total = total + slot[...].astype(F32)
            return total

        def drain():
            for way, buf, sends in ((1, buf_p, p_s), (-1, buf_m, m_s)):
                count = sum(length(way, h) for h in range(pieces))
                if count:
                    sent(buf.at[:count], sends)

        return begin, step_of, result, drain

    copies = []
    for q in range(quads):
        copies += to_sibling(pp, psib, psib_send, psib_recv, q, cols)
    for copy in copies:
        copy.start()
    begin, step_of, result, drain_projection = reduce_scatter(
        pp,
        psib,
        pst,
        prp,
        prm,
        (psib_recv, prp_send, prp_recv, prm_send, prm_recv),
        2,
        cols,
    )
    begin()

    def projection_step(j, _):
        step_of(j)
        return 0

    lax.fori_loop(2, hops + 1, projection_step, 0)
    parts = [result(h) for h in range(2)]
    got(sqb.at[: n_tp - 1], sq_recv)
    squares = sqb[0]
    for t in range(1, n_tp):
        squares = squares + sqb[t]
    inverse = lax.rsqrt(squares / (n_tp * LANES) + EPSILON)
    inverse = column_of(inverse, q_me * tokens, tokens)
    loads[1].wait()
    for h in range(2):
        at = slice(h * half_tokens, (h + 1) * half_tokens)
        resid[at, :] = (
            resid[at, :].astype(F32) + parts[h] * inverse[at, :]
        ).astype(BF16)
    after = resid[...].astype(F32)
    sq2[pl.ds(p_me, 1), :, :] = row_of(
        jnp.sum(after * after, axis=1, keepdims=True), LANES
    ).reshape(1, 1, LANES)

    def quad_peer(d):
        return lax.rem(p_me + d, PARTS)

    def norm_copy(d, source):
        return remote(
            sq2.at[source],
            sq2.at[source],
            s2_send,
            s2_recv,
            tp=q_me * PARTS + quad_peer(d),
        )

    for d in range(1, PARTS):
        norm_copy(d, p_me).start()

    scale = fgain[:, cols(p_me)]
    got(sq2.at[: PARTS - 1], s2_recv)
    squares = sq2[0] + sq2[1] + sq2[2] + sq2[3]
    inverse = column_of(lax.rsqrt(squares / model + EPSILON), 0, tokens)
    normed = (after * inverse * scale).astype(BF16)
    turn = 2 * lax.rem(z_me, 2) - 1

    def quad_at(k):
        far = lax.div(k, 2)
        offset = jnp.where(lax.rem(k, 2) == 0, turn * far, -turn * far)
        return lax.rem(q_me + offset + 2 * quads, quads)

    xa[z_me] = normed[:, half_w:]

    def ahead_copy(direction, k, chip):
        sends, recvs = (xap_send, xap_recv) if direction > 0 else (xam_send, xam_recv)
        return remote(
            xa.at[chip],
            xa.at[chip],
            sends,
            recvs.at[k],
            tp=up if direction > 0 else down,
        )

    def ahead_step(k):
        for direction, n in ((1, hops), (-1, hops - 1)):

            def arrive(direction=direction, n=n):
                chip = chip_at(-direction * k)
                ahead_copy(direction, k - 1, chip).wait_recv()
                when(k < n, lambda: ahead_copy(direction, k, chip).start())

            when(k <= n, arrive)

    ahead_copy(1, 0, z_me).start()
    if hops > 1:
        ahead_copy(-1, 0, z_me).start()

    over_slots = (((0,), (0,)), ((), ()))
    outgoing = lax.dot_general(
        pk[q_me], normed[:, :half_w], over_slots, preferred_element_type=F32
    ).astype(BF16)
    og[...] = outgoing.reshape(n_sp, slot_rows, half_w)
    xg[q_me, rows(s_me * slot_rows, slot_rows), z_cols(p_me)] = og[s_me]

    def dispatch_copy(d, source, peer):
        return remote(
            og.at[peer],
            xg.at[q_me, rows(source * slot_rows, slot_rows), z_cols(p_me)],
            di_send,
            di_recv.at[lax.div(source, n_sp // PIECES)],
            sp=peer,
        )

    for d in range(1, n_sp):
        dispatch_copy(d, s_me, sp_peer(d)).start()

    def late_copy(q, d, source, peer):
        return remote(
            ox.at[q, peer],
            xg.at[q, rows(source * slot_rows, slot_rows), x_cols(c_me)],
            ox_send.at[q],
            ox_recv.at[q],
            sp=peer,
        )

    def send_quad(q):
        both = jnp.concatenate([xa[2 * q], xa[2 * q + 1]], axis=1)
        picked = lax.dot_general(pk[q], both, over_slots, preferred_element_type=F32)
        ox[q] = picked.astype(BF16).reshape(n_sp, slot_rows, width)
        xg[q, rows(s_me * slot_rows, slot_rows), x_cols(c_me)] = ox[q, s_me]

        def one(d, _):
            late_copy(q, d, s_me, sp_peer(d)).start()
            return 0

        lax.fori_loop(1, n_sp, one, 0)

    def sub_block(chip, h, core):
        return xg.at[
            lax.div(chip, 2),
            pl.ds(h * piece_slots, piece_slots),
            z_cols(lax.rem(chip, 2) * 2 + core),
        ]

    def ring_copy(direction, h, k, chip):
        sends, recvs = (agp_send, agp_recv) if direction > 0 else (agm_send, agm_recv)
        view = sub_block(chip, h, c_me)
        return remote(
            view, view, sends, recvs.at[h, k], tp=up if direction > 0 else down
        )

    def across_copy(h, chip, core):
        view = sub_block(chip, h, core)
        return remote(view, view, ags_send, ags_recv.at[lax.div(chip, 2)], tp=sibling)

    def across_late(q, core):
        view = xg.at[q, :, x_cols(core)]
        return remote(view, view, ags_send, ags_recv.at[q], tp=sibling)

    def reach(direction, h):
        return hops if (direction > 0) == (h % 2 == 0) else hops - 1

    ahead_step(1)
    send_quad(quad_at(1))
    ahead_step(2)
    send_quad(quad_at(2))
    for h in range(PIECES):
        group = n_sp // PIECES
        mine = lax.div(s_me, group) == h

        @pl.when(jnp.logical_not(mine))
        def _(h=h, group=group):
            got(og.at[:group], di_recv.at[h])

        if group > 1:

            @pl.when(mine)
            def _(h=h, group=group):
                got(og.at[: group - 1], di_recv.at[h])

        for direction in (1, -1):
            if reach(direction, h):
                ring_copy(direction, h, 0, z_me).start()
        across_copy(h, z_me, c_me).start()
    pltpu.make_async_copy(wgu, wgu, load_sem.at[2]).wait()
    pltpu.make_async_copy(wd, wd, load_sem.at[3]).wait()

    def forward(k, h):
        for direction in (1, -1) if h % 2 == 0 else (-1, 1):
            n = reach(direction, h)

            def arrive(direction=direction, n=n):
                chip = chip_at(-direction * k)
                ring_copy(direction, h, k - 1, chip).wait_recv()

                @pl.when(k < n)
                def _():
                    ring_copy(direction, h, k, chip).start()

                across_copy(h, chip, c_me).start()

            pl.when(k <= n)(arrive)

    def forward_late(q):
        got(ox.at[q, : n_sp - 1], ox_recv.at[q])
        across_late(q, c_me).start()

    def late_to_sibling(q):
        return remote(
            po.at[q, :, x_cols(1 - c_me)],
            xsib.at[q],
            xsib_send,
            xsib_recv.at[q],
            tp=sibling,
        )

    def out_to_sibling(q):
        return [late_to_sibling(q)] + to_sibling(po, sib, sib_send, sib_recv, q, z_cols)

    def experts_gate(q):
        got(xg.at[q, :, : model // 2], ags_recv.at[q])
        both = jnp.dot(xg[q], wgu[...], preferred_element_type=F32)
        gs[...] = (jax.nn.silu(both[:, :units_n]) * both[:, units_n:]).astype(BF16)

    def experts(q):
        units = gs[...]
        for part in range(PARTS):
            at = slice(part * width, (part + 1) * width)
            po[q, :, at] = jnp.dot(units, wd[:, at], preferred_element_type=F32).astype(BF16)
        for copy in out_to_sibling(q):
            copy.start()

    def early_copy(q, d, source, peer):
        return remote(
            xo.at[q, peer], xi.at[q, source], xo_send.at[q], xo_recv.at[q], sp=peer
        )

    def return_early(q):
        late_to_sibling(q).wait_recv()
        total = po[q, :, x_cols(c_me)].astype(F32) + xsib[q].astype(F32)
        xo[q] = total.astype(BF16).reshape(n_sp, slot_rows, width)
        xi[q, pl.ds(s_me, 1)] = xo[q, pl.ds(s_me, 1)]

        def one(d, _):
            early_copy(q, d, s_me, sp_peer(d)).start()
            return 0

        lax.fori_loop(1, n_sp, one, 0)

    def weigh(q, back):
        return jnp.dot(wh[q], back, preferred_element_type=F32) + jnp.dot(
            wl[q], back, preferred_element_type=F32
        )

    def home_copy(chip):
        return remote(
            co.at[chip], ci.at[z_me], co_send, co_recv, tp=chip * 2 + c_me
        )

    def home_result():
        got(ci.at[: n_z - 1], co_recv)
        total = co[z_me].astype(F32)
        for d in range(1, n_z):
            total = total + ci[chip_at(d)].astype(F32)
        return total

    def weigh_early(q):
        got(xi.at[q, : n_sp - 1], xo_recv.at[q])
        total = weigh(q, xi[q].reshape(slots, width))
        for j in range(2):
            chip = 2 * q + j
            co[chip] = total[:, j * half_w : (j + 1) * half_w].astype(BF16)

            @pl.when(chip != z_me)
            def _(chip=chip):
                home_copy(chip).start()


    def gather_step(k, _):
        @pl.when(k <= hops - 2)
        def _():
            ahead_step(k + 2)
            send_quad(quad_at(k + 2))

        @pl.when(k <= hops)
        def _():
            for h in range(PIECES // 2):
                forward(k, h)

        @pl.when(k >= 2)
        def _():
            experts_gate(quad_at(k - 1))

        @pl.when(k <= hops)
        def _():
            for h in range(PIECES // 2, PIECES):
                forward(k, h)
            forward_late(quad_at(k))

        @pl.when(k >= 2)
        def _():
            experts(quad_at(k - 1))

        @pl.when(k >= 3)
        def _():
            return_early(quad_at(k - 2))

        return 0

    lax.fori_loop(1, hops + 2, gather_step, 0)

    begin, step_of, result, drain_experts = reduce_scatter(
        po,
        sib,
        st,
        rp,
        rm,
        (sib_recv, rp_send, rp_recv, rm_send, rm_recv),
        PIECES,
        z_cols,
    )
    begin()
    return_early(quad_at(hops))

    weighed = 0
    for j in range(2, hops + 1):
        step_of(j)
        upto = hops if j == hops else min(2 * j - 3, hops)
        for k in range(weighed + 1, upto + 1):
            weigh_early(quad_at(k))
        weighed = upto
    piece_sp = n_sp // PIECES

    def return_copy(d, source, peer):
        return remote(
            ret.at[peer], rt.at[source], ret_send, ret_recv, sp=peer
        )

    for h in range(PIECES):
        ret[h * piece_sp : (h + 1) * piece_sp] = (
            result(h).astype(BF16).reshape(piece_sp, slot_rows, half_w)
        )
    rt[pl.ds(s_me, 1)] = ret[pl.ds(s_me, 1)]
    for d in range(1, n_sp):
        return_copy(d, s_me, sp_peer(d)).start()
    got(rt.at[: n_sp - 1], ret_recv)
    routed = weigh(q_me, rt[...].reshape(slots, half_w))
    fo[:, :, :half_w] = (
        (resid[:, :half_w].astype(F32) + routed)
        .astype(BF16)
        .reshape(PARTS, ROUTE_ROWS, half_w)
    )
    routed = home_result()
    fo[:, :, half_w:] = (
        (resid[:, half_w:].astype(F32) + routed)
        .astype(BF16)
        .reshape(PARTS, ROUTE_ROWS, half_w)
    )
    fin[pl.ds(p_me, 1)] = fo[pl.ds(p_me, 1)]

    def final_copy(d, source, peer):
        return remote(
            fo.at[peer],
            fin.at[source],
            fin_send,
            fin_recv,
            tp=q_me * PARTS + peer,
        )

    for d in range(1, PARTS):
        final_copy(d, p_me, quad_peer(d)).start()
    sent(rx.at[: (n_sp - 1) * 16, :], fr_send)
    sent(sqb.at[: n_tp - 1], sq_send)
    sent(psib, psib_send)
    drain_projection()
    sent(sq2.at[: PARTS - 1], s2_send)
    sent(xa.at[:hops], xap_send)
    if hops > 1:
        sent(xa.at[: hops - 1], xam_send)
    sent(og.at[: n_sp - 1], di_send)
    hop_count = PIECES // 2 * (2 * hops - 1)
    sent(rp.at[:hop_count], agp_send)
    sent(rm.at[:hop_count], agm_send)
    sent(xg.at[:2], ags_send) if quads == 4 else sent(xg, ags_send)
    for q in range(quads):
        sent(ox.at[q, : n_sp - 1], ox_send.at[q])
        sent(xo.at[q, : n_sp - 1], xo_send.at[q])
    sent(sib, sib_send)
    sent(xsib, xsib_send)
    drain_experts()
    sent(co.at[: n_z - 1], co_send)
    sent(ret.at[: n_sp - 1], ret_send)
    got(fin.at[: PARTS - 1], fin_recv)
    for part in range(PARTS):
        out[:, part * width : (part + 1) * width] = fin[part]
    sent(fo.at[: PARTS - 1], fin_send)


def local(
    n_sp,
    n_tp,
    lru_input,
    gate_input,
    documents,
    conv_taps,
    rate_weight,
    inlet_weight,
    decay_param,
    lru_gain,
    out_weight,
    residual,
    ffn_gain,
    routes,
    route_weights,
    w_gate,
    w_up,
    w_down,
):
    positions, channels = lru_input.shape
    model = residual.shape[1]
    units = w_gate.shape[2]
    width = model // PARTS
    half_w = width // 2
    n_z = n_tp // 2
    hops = n_z // 2
    quads = n_tp // PARTS
    tokens = positions // quads
    cap = 2 * routes.shape[1] * ROUTE_ROWS // n_sp
    slot_rows = PARTS * cap
    block_rows = n_sp * slot_rows
    pitch = positions + 64
    vmem = pl.BlockSpec(memory_space=pltpu.VMEM)
    hbm = pl.BlockSpec(memory_space=pl.ANY)
    dma = pltpu.SemaphoreType.DMA
    scratch = [
        pltpu.VMEM(lru_input.shape, BF16),
        pltpu.VMEM(gate_input.shape, BF16),
        pltpu.VMEM((1, positions), jnp.int32),
        pltpu.VMEM(conv_taps.shape, BF16),
        pltpu.VMEM(rate_weight.shape[1:], BF16),
        pltpu.VMEM(inlet_weight.shape[1:], BF16),
        pltpu.VMEM((1, channels), F32),
        pltpu.VMEM((1, channels), F32),
        pltpu.VMEM((1, model), F32),
        pltpu.VMEM((2, positions), jnp.int32),
        pltpu.VMEM((2, positions), F32),
        dma((11,)),
        pltpu.VMEM((positions + 8, LANES), F32),
        pltpu.VMEM((positions + 8, LANES), F32),
        pltpu.VMEM((pitch, LANES), F32),
        pltpu.VMEM((pitch, LANES), F32),
        pltpu.VMEM((positions, LANES), F32),
        pltpu.VMEM(((n_sp + 1) * 16, LANES), F32),
        pltpu.VMEM((2 * n_sp, LANES), F32),
        pltpu.VMEM((6 * n_sp, LANES), F32),
        pltpu.VMEM((channels, model), BF16),
        pltpu.VMEM((tokens, width), BF16),
        pltpu.VMEM((model, 2 * units), BF16),
        pltpu.VMEM((units, model), BF16),
        pltpu.VMEM((n_tp, 1, positions), F32),
        pltpu.VMEM((PARTS, 1, LANES), F32),
        pltpu.VMEM((quads, tokens, model), BF16),
        pltpu.VMEM((n_z, tokens, width), BF16),
        pltpu.VMEM((4, tokens // 2, width), BF16),
        pltpu.VMEM((2 * hops, tokens // 2, width), BF16),
        pltpu.VMEM((2 * hops, tokens // 2, width), BF16),
        pltpu.VMEM((quads, tokens, block_rows), BF16),
        pltpu.VMEM((quads, tokens, block_rows), BF16),
        pltpu.VMEM((quads, tokens, block_rows), BF16),
        pltpu.VMEM((n_sp, slot_rows, half_w), BF16),
        pltpu.VMEM((n_z, tokens, half_w), BF16),
        pltpu.VMEM((quads, n_sp, slot_rows, width), BF16),
        pltpu.VMEM((quads, block_rows, model), BF16),
        pltpu.VMEM((quads, block_rows, model), BF16),
        pltpu.VMEM((n_z, block_rows, half_w), BF16),
        pltpu.VMEM((quads, block_rows, width), BF16),
        pltpu.VMEM((quads, n_sp, slot_rows, width), BF16),
        pltpu.VMEM((quads, n_sp, slot_rows, width), BF16),
        pltpu.VMEM((n_z, tokens, half_w), BF16),
        pltpu.VMEM((n_z, tokens, half_w), BF16),
        pltpu.VMEM((block_rows, units), BF16),
        pltpu.VMEM((2 * PIECES, block_rows // PIECES, half_w), BF16),
        pltpu.VMEM((PIECES * hops, block_rows // PIECES, half_w), BF16),
        pltpu.VMEM((PIECES * hops, block_rows // PIECES, half_w), BF16),
        pltpu.VMEM((n_sp, slot_rows, half_w), BF16),
        pltpu.VMEM((n_sp, slot_rows, half_w), BF16),
        pltpu.VMEM((PARTS, ROUTE_ROWS, width), BF16),
        pltpu.VMEM((PARTS, ROUTE_ROWS, width), BF16),
        dma((4,)),
        dma(()),
        dma(()),
        dma(()),
        dma(()),
        dma(()),
        dma(()),
        dma(()),
        dma((quads,)),
        dma(()),
        dma((2, hops)),
        dma(()),
        dma((2, hops)),
        dma(()),
        dma((PIECES,)),
        dma(()),
        dma((PIECES, hops)),
        dma(()),
        dma((PIECES, hops)),
        dma(()),
        dma((quads,)),
        dma(()),
        dma((hops,)),
        dma(()),
        dma((hops,)),
        dma((quads,)),
        dma((quads,)),
        dma(()),
        dma((quads,)),
        dma(()),
        dma((quads,)),
        dma((quads,)),
        dma((quads,)),
        dma(()),
        dma(()),
        dma(()),
        dma((PIECES, hops)),
        dma(()),
        dma((PIECES, hops)),
        dma(()),
        dma(()),
        dma(()),
        dma(()),
    ]
    return pl.pallas_call(
        functools.partial(kernel, n_sp, n_tp),
        out_shape=jax.ShapeDtypeStruct((positions // n_tp, model), BF16),
        in_specs=[hbm] * 16,
        out_specs=vmem,
        scratch_shapes=scratch,
        name="layer",
        compiler_params=pltpu.CompilerParams(
            collective_id=0, has_side_effects=True, vmem_limit_bytes=56 * 1024 * 1024
        ),
    )(
        lru_input,
        gate_input,
        documents.reshape(1, positions),
        conv_taps,
        rate_weight[0],
        inlet_weight[0],
        decay_param.reshape(1, channels),
        lru_gain.reshape(1, channels),
        ffn_gain.reshape(1, model),
        routes.T,
        route_weights.T,
        out_weight,
        residual,
        w_gate[0],
        w_up[0],
        w_down[0],
    )


def solution(mesh):
    return jax.shard_map(
        functools.partial(local, mesh.shape["sp"], mesh.shape["tp"]),
        mesh=mesh,
        in_specs=(
            P("sp", "tp"),
            P("sp", "tp"),
            P("sp"),
            P(None, "tp"),
            P("tp", None, None),
            P("tp", None, None),
            P("tp"),
            P("tp"),
            P("tp", None),
            P("sp", None),
            P(),
            P("sp", None),
            P("sp", None),
            P("sp", None, "tp"),
            P("sp", None, "tp"),
            P("sp", "tp", None),
        ),
        out_specs=P(("sp", "tp"), None),
        check_vma=False,
    )
```
